32 devices in a mesh: sp: 8 (over z, y), dp: 4 (over x, core).
Axes of the slice: x: 2, y: 2, z: 4, core: 2. Of those that a mesh axis runs over, the one named last changes fastest.
Arguments:
- tokens: bfloat16 [4, 1024, 2048], P('dp', 'sp'), may hold values from -6 to 6
- cotangent: bfloat16 [4, 1024, 2048], P('dp', 'sp'), may hold values from -6 to 6
- value_weight: bfloat16 [2048, 2048], P(('sp', 'dp')), may hold values from -0.125 to 0.125
- query_heads: bfloat16 [4, 1024, 16, 128], P('dp', None, 'sp'), may hold values from -8 to 8
- key_heads: bfloat16 [4, 1024, 16, 128], P('dp', None, 'sp'), may hold values from -8 to 8
- lambdas: float32 [16], P('sp'), may hold values from 0.3 to 0.8
Outputs:
- grad_query: bfloat16 [4, 1024, 16, 128], P('dp', None, 'sp')
- grad_key: bfloat16 [4, 1024, 16, 128], P('dp', None, 'sp')
- grad_tokens: bfloat16 [4, 1024, 2048], P('dp', 'sp')
- grad_value_weight: float32 [2048, 2048], P(('sp', 'dp'))
- grad_lambda: float32 [16], P('sp')
The draws below stay inside these ranges and needn't reach their ends.
All inputs are finite; a program needn't handle non-finite values.
Results may differ from the reference program's by a relative error of at most 0.0095.
Values may be sent and summed in bfloat16 or wider, within the bound.
A program may use at most 192 MiB of HBM per device.

```python
import jax
import jax.numpy as jnp
from jax import lax

D = 2048
HEADS = 16
HEAD_DIM = 64
QBLOCK = 256
SEQS = 4
LENGTH = 1024
FEATURES = 2048


def pair_heads(key):
    array_shape = (SEQS, LENGTH, HEADS, 2 * HEAD_DIM)
    key_first = jax.random.fold_in(key, 11)
    key_second = jax.random.fold_in(key, 12)
    keys_part = jnp.clip(jax.random.normal(key_first, array_shape, jnp.float32) * 1.32, -8.0, 8.0)
    query_part = jnp.clip(jax.random.normal(key_second, array_shape, jnp.float32) * 1.32, -8.0, 8.0)
    return (query_part, keys_part)


def draw_query_heads(key, part):
    return pair_heads(key)[0].astype(jnp.bfloat16)


def draw_key_heads(key, part):
    return pair_heads(key)[1].astype(jnp.bfloat16)


def spiked(array, own_key, source, target, blocks, factor):
    def block_of(position):
        return (jnp.arange(array.shape[position]) // (array.shape[position] // blocks)).reshape((-1,) + (1,) * (array.ndim - 1 - position))

    first = jax.random.permutation(own_key, blocks)[block_of(target)]
    second = (block_of(target) + blocks // 2) % blocks
    return jnp.where((block_of(source) == first) | (block_of(source) == second), factor * array, array)


def block_levels(stream_key, shape, split, smallest, top_value):
    level, own = 1.0, jax.random.fold_in(stream_key, 6)
    for dim, blocks in split:
        steps = jnp.exp(jax.random.uniform(jax.random.fold_in(own, dim), (blocks,), jnp.float32, smallest / len(split), top_value / len(split)))
        level = level * jnp.repeat(steps, shape[dim] // blocks).reshape([-1 if axis == dim else 1 for axis in range(len(shape))])
    return level


def noise(own_key, shape, spread, limit, split=(), held_as=jnp.bfloat16):
    loudness = block_levels(own_key, shape, split, -0.22, 0.18) if split else 1.0
    values = jax.random.normal(own_key, shape, jnp.float32) * spread * loudness
    return jnp.minimum(jnp.maximum(values, -limit), limit).astype(held_as)


def bell_draw_with(rng, dims, deviation, reach, cuts, heavy, kind=jnp.bfloat16):
    drawn = deviation * jax.random.normal(rng, dims, jnp.float32)
    if cuts:
        drawn = drawn * block_levels(rng, dims, cuts, -0.22, 0.18)
    return jnp.clip(spiked(drawn, jax.random.fold_in(rng, 3), *heavy), -reach, reach).astype(kind)


def setup_inputs(seed: int = 0) -> dict:
    key_of = jax.random.split(jax.random.key(seed), 7)
    tokens = bell_draw_with(key_of[0], (SEQS, LENGTH, D), 1.0, 6.0, ((0, 4), (1, 8)), (1, 2, 8, 2.0))
    cotangent = noise(key_of[1], (SEQS, LENGTH, FEATURES), 1.0, 6.0, ((0, 4), (1, 8)))
    value_weight = noise(key_of[2], (D, FEATURES), D ** -0.5, 0.125, ((0, 32),))
    query_heads = draw_query_heads(jax.random.fold_in(key_of[6], 71), 0)
    key_heads = draw_key_heads(jax.random.fold_in(key_of[6], 71), 0)
    lambdas = jnp.clip(0.3 + 0.5 * jax.random.uniform(key_of[5], (HEADS,), jnp.float32) ** block_levels(key_of[5], (HEADS,), ((0, 8),), -0.2, 0.2), 0.3, 0.8)
    return {"tokens": tokens, "cotangent": cotangent, "value_weight": value_weight, "query_heads": query_heads, "key_heads": key_heads, "lambdas": lambdas}


EPS = 1e-06
NEGATIVE = -1e+30

def head_backward(queries, keys_in, values_in, cotangent, lambdas, block_rows):
    seq_length = queries.shape[0]
    head_count = queries.shape[1]
    head_width = queries.shape[3]
    scaling = head_width ** (-0.5)
    blocks_count = seq_length // block_rows
    positions = jnp.arange(seq_length, dtype=jnp.int32)
    keys_wide = keys_in.astype(jnp.float32)
    values_wide = values_in.astype(jnp.float32)
    lambda_col = lambdas[:, None, None]

    def block_step(totals, block_index):
        grad_key_sum, grad_value_sum, grad_lambda_sum = totals
        offset = (block_index * block_rows).astype(jnp.int32)
        query_block = lax.dynamic_slice_in_dim(queries, offset, block_rows, 0).astype(jnp.float32)
        cotan_block = lax.dynamic_slice_in_dim(cotangent, offset, block_rows, 0).astype(jnp.float32)
        scores = jnp.einsum('qhcd,khcd->hcqk', query_block, keys_wide) * scaling
        rows_pos = offset + jnp.arange(block_rows, dtype=jnp.int32)
        allowed = rows_pos[:, None] >= positions[None, :]
        scores = jnp.where(allowed, scores, NEGATIVE)
        highest = lax.optimization_barrier(jnp.max(scores, axis=-1, keepdims=True))
        exponent = jnp.exp(scores - highest)
        softmaxes = exponent / lax.optimization_barrier(jnp.sum(exponent, axis=-1, keepdims=True))
        weights = (softmaxes[:, 0] - lambda_col * softmaxes[:, 1]).astype(jnp.bfloat16)
        weights_wide = weights.astype(jnp.float32)
        mixed_out = jnp.einsum('hqk,khd->qhd', weights_wide, values_wide)
        inverse = lax.rsqrt(lax.optimization_barrier(jnp.mean(mixed_out * mixed_out, axis=-1, keepdims=True)) + EPS)
        normed = mixed_out * inverse
        grad_mixed = (inverse * (cotan_block - normed * lax.optimization_barrier(jnp.mean(cotan_block * normed, axis=-1, keepdims=True)))).astype(jnp.bfloat16)
        grad_mixed_wide = grad_mixed.astype(jnp.float32)
        grad_weights = jnp.einsum('qhd,khd->hqk', grad_mixed_wide, values_wide)
        grad_value_sum = grad_value_sum + jnp.einsum('hqk,qhd->khd', weights_wide, grad_mixed_wide)
        grad_lambda_sum = grad_lambda_sum - lax.optimization_barrier(jnp.sum(grad_weights * softmaxes[:, 1], axis=(1, 2)))
        first_grad = softmaxes[:, 0] * (grad_weights - lax.optimization_barrier(jnp.sum(grad_weights * softmaxes[:, 0], axis=-1, keepdims=True)))
        second_grad = -lambda_col * softmaxes[:, 1] * (grad_weights - lax.optimization_barrier(jnp.sum(grad_weights * softmaxes[:, 1], axis=-1, keepdims=True)))
        grad_scores = (jnp.stack([first_grad, second_grad], axis=1) * scaling).astype(jnp.bfloat16)
        grad_scores_wide = grad_scores.astype(jnp.float32)
        grad_query_block = jnp.einsum('hcqk,khcd->qhcd', grad_scores_wide, keys_wide).astype(jnp.bfloat16)
        grad_key_sum = grad_key_sum + jnp.einsum('hcqk,qhcd->khcd', grad_scores_wide, query_block)
        return ((grad_key_sum, grad_value_sum, grad_lambda_sum), grad_query_block)
    initial = (jnp.zeros(keys_in.shape, jnp.float32), jnp.zeros(values_in.shape, jnp.float32), jnp.zeros((head_count,), jnp.float32))
    totals, query_blocks = lax.scan(block_step, initial, jnp.arange(blocks_count, dtype=jnp.int32))
    grad_query = query_blocks.reshape(queries.shape)
    return (grad_query, totals[0].astype(jnp.bfloat16), totals[1].astype(jnp.bfloat16), totals[2])

def reference(tokens, cotangent, value_weight, query_heads, key_heads, lambdas):
    seq_count = tokens.shape[0]
    seq_length = tokens.shape[1]
    feature_count = value_weight.shape[1]
    flat_tokens = tokens.reshape(seq_count * seq_length, D)
    values_flat = jnp.dot(flat_tokens, value_weight, preferred_element_type=jnp.float32).astype(jnp.bfloat16)
    values_heads = values_flat.reshape(seq_count, seq_length, HEADS, 2 * HEAD_DIM)
    cotan_heads = cotangent.reshape(seq_count, seq_length, HEADS, 2 * HEAD_DIM)
    queries = query_heads.reshape(seq_count, seq_length, HEADS, 2, HEAD_DIM)
    keys_in = key_heads.reshape(seq_count, seq_length, HEADS, 2, HEAD_DIM)

    def one_sequence(items):
        return head_backward(items[0], items[1], items[2], items[3], lambdas, QBLOCK)
    grad_query, grad_key, grad_value, grad_lambda = lax.map(one_sequence, (queries, keys_in, values_heads, cotan_heads))
    grad_lambda = lax.optimization_barrier(jnp.sum(grad_lambda, axis=0))
    grad_flat = grad_value.reshape(seq_count * seq_length, feature_count)
    grad_tokens = jnp.dot(grad_flat, value_weight.T, preferred_element_type=jnp.float32).astype(jnp.bfloat16)
    grad_weight = jnp.dot(flat_tokens.T, grad_flat, preferred_element_type=jnp.float32)
    return (grad_query.reshape(query_heads.shape), grad_key.reshape(key_heads.shape), grad_tokens.reshape(tokens.shape), grad_weight, grad_lambda)
```

```python
import functools

import jax
import jax.numpy as jnp
from jax import lax
from jax.experimental import pallas as pl
from jax.experimental.pallas import tpu as pltpu
from jax.sharding import PartitionSpec as P

QBLOCK = 256
EPS = 1e-06
NEGATIVE = -1e30
CHUNKS = 4
F32 = jnp.float32
BF16 = jnp.bfloat16


def dot_nn(a, b):
    return jnp.dot(a, b, preferred_element_type=F32)


def dot_nt(a, b):
    return lax.dot_general(a, b, (((1,), (1,)), ((), ())), preferred_element_type=F32)


def remote(src, dst, send, recv, sp, dp):
    return pltpu.make_async_remote_copy(
        src_ref=src,
        dst_ref=dst,
        send_sem=send,
        recv_sem=recv,
        device_id=(sp, dp),
        device_id_type=pl.DeviceIdType.MESH,
    )


def greet(peers):
    barrier = pltpu.get_barrier_semaphore()
    for sp, dp in peers:
        pl.semaphore_signal(
            barrier, inc=1, device_id=(sp, dp), device_id_type=pl.DeviceIdType.MESH
        )
    pl.semaphore_wait(barrier, len(peers))


class Attention:
    def __init__(self, lam_ref, q_ref, k_ref, v_ref, g_ref, bufs, outs, width):
        self.lam_ref, self.q_ref, self.k_ref = lam_ref, q_ref, k_ref
        self.v_ref, self.g_ref, self.width = v_ref, g_ref, width
        self.p_ref, self.a_ref, self.qh_ref, self.kt_ref, self.go_ref = bufs[:5]
        self.gv_acc, self.gk_acc = bufs[5:]
        self.gq_ref, self.gk_ref, self.gl_ref = outs
        self.length = q_ref.shape[0]
        self.block = min(QBLOCK, self.length)
        self.count = self.length // self.block

    def span(self, index):
        off = index * self.block
        reach = off + self.block
        pieces = ([(0, off)] if off else []) + [(off, reach)]
        base = self.block * (index * (index + 1) // 2)
        return off, reach, pieces, base

    def columns(self, head):
        return slice(head * self.width, (head + 1) * self.width)

    def prepare(self, head):
        length, width = self.length, self.width
        half = width // 2
        scaling = half ** (-0.5)
        lanes = lax.broadcasted_iota(jnp.int32, (length, width), 1)
        first_half = lanes < half
        q_all = self.q_ref[:, self.columns(head)].astype(F32) * scaling
        k_all = self.k_ref[:, self.columns(head)].astype(F32) * scaling
        self.qh_ref[head, 0] = jnp.where(first_half, q_all, 0.0).astype(BF16)
        self.qh_ref[head, 1] = jnp.where(first_half, 0.0, q_all).astype(BF16)
        self.kt_ref[head, 0] = jnp.where(first_half, k_all, 0.0).T.astype(BF16)
        self.kt_ref[head, 1] = jnp.where(first_half, 0.0, k_all).T.astype(BF16)

    def softmaxes(self, head, index):
        block = self.block
        lam = self.lam_ref[head]
        keep = lax.broadcasted_iota(jnp.int32, (block, block), 0) <= lax.broadcasted_iota(
            jnp.int32, (block, block), 1
        )
        off, reach, pieces, base = self.span(index)
        probs = []
        for c in range(2):
            qc = self.qh_ref[head, c, off:reach]
            scores = [dot_nt(self.k_ref[lo:hi, self.columns(head)], qc) for lo, hi in pieces]
            scores[-1] = jnp.where(keep, scores[-1], NEGATIVE)
            top = functools.reduce(
                jnp.maximum, [jnp.max(s, axis=0, keepdims=True) for s in scores]
            )
            exps = [jnp.exp(s - top) for s in scores]
            total = sum(jnp.sum(e, axis=0, keepdims=True) for e in exps)
            inv = 1.0 / total
            probs.append([e * inv for e in exps])
            for (lo, hi), p in zip(pieces, probs[c]):
                self.p_ref[head, c, base + lo : base + hi] = p
        for (lo, hi), p1, p2 in zip(pieces, *probs):
            self.a_ref[head, base + lo : base + hi] = (p1 - lam * p2).astype(BF16)

    def values_grad(self, head):
        width = self.width
        v_all = self.v_ref[:, :, :, self.columns(head)].reshape(self.length, width)
        vt = v_all.astype(F32).T.astype(BF16)
        gt = self.g_ref[:, :, self.columns(head)].reshape(self.length, width).astype(F32).T
        for index in range(self.count):
            off, reach, pieces, base = self.span(index)
            weights = self.a_ref[head, base : base + reach]
            out_t = dot_nn(vt[:, :reach], weights)
            cot = gt[:, off:reach]
            inverse = lax.rsqrt(jnp.mean(out_t * out_t, axis=0, keepdims=True) + EPS)
            normed = out_t * inverse
            grad_out = (
                inverse * (cot - normed * jnp.mean(cot * normed, axis=0, keepdims=True))
            ).astype(BF16)
            self.go_ref[head, :, off:reach] = grad_out
            gv = dot_nt(weights, grad_out)
            if off:
                self.gv_acc[0:off] += gv[0:off]
            self.gv_acc[off:reach] = gv[off:reach]

    def scores_grad(self, head):
        block, width = self.block, self.width
        lam = self.lam_ref[head]
        v_all = self.v_ref[:, :, :, self.columns(head)].reshape(self.length, width)
        lambda_total = jnp.zeros((1, block), F32)
        for index in range(self.count):
            off, reach, pieces, base = self.span(index)
            grad_out = self.go_ref[head, :, off:reach]
            probs = [
                [self.p_ref[head, c, base + lo : base + hi] for lo, hi in pieces]
                for c in range(2)
            ]
            grad_w = [dot_nn(v_all[lo:hi], grad_out) for lo, hi in pieces]
            sums = [
                sum(jnp.sum(d * p, axis=0, keepdims=True) for d, p in zip(grad_w, probs[c]))
                for c in range(2)
            ]
            lambda_total = lambda_total - sums[1]
            first = [(p * (d - sums[0])).astype(BF16) for d, p in zip(grad_w, probs[0])]
            second = [(-lam * p * (d - sums[1])).astype(BF16) for d, p in zip(grad_w, probs[1])]
            gq_t = sum(
                dot_nn(self.kt_ref[head, 0, :, lo:hi], a)
                + dot_nn(self.kt_ref[head, 1, :, lo:hi], b)
                for (lo, hi), a, b in zip(pieces, first, second)
            )
            self.gq_ref[off:reach, self.columns(head)] = gq_t.T.astype(BF16)
            for (lo, hi), a, b in zip(pieces, first, second):
                gk = dot_nn(a, self.qh_ref[head, 0, off:reach]) + dot_nn(
                    b, self.qh_ref[head, 1, off:reach]
                )
                if lo == off:
                    self.gk_acc[lo:hi, :] = gk
                else:
                    self.gk_acc[lo:hi, :] += gk
        self.gk_ref[:, self.columns(head)] = self.gk_acc[...].astype(BF16)
        self.gl_ref[head] = jnp.broadcast_to(
            jnp.sum(lambda_total, axis=1, keepdims=True), self.gl_ref.shape[1:]
        )


def whole_kernel(
    n, m, width,
    lam_ref, tok_ref, cot_ref, w_ref, q_ref, k_ref,
    gq_ref, gk_ref, gt_ref, gw_ref, glo_ref,
    tokens, tok_t, wc, coth, vloc, v_ref, p_ref, a_ref, qh_ref, kt_ref, go_ref, gv_acc, gk_acc,
    gvb, dv, part, ry, sz, rz, term, ra, sa, rb, sb, rc, sc, rd, gl_ref, lbuf,
    local_sem, wa_s, wa_r, wb_s, wb_r, wx_s, wx_r, wd_s, wd_r, tz_s, tz_r, ty_s, ty_r,
    c_s, c_r, v_s, v_r, dv_s, dv_r, y_s, y_r, z_s, z_r, a_s, a_r, b_s, b_r, e_s, e_r,
    d_s, d_r, l_s, l_r,
):
    me = lax.axis_index("sp")
    dp = lax.axis_index("dp")
    place = n // 2
    levels = place // 2
    spans = m // 2
    half, pos = me // place, me % place
    level, y = pos // 2, pos % 2
    x, core = dp // 2, dp % 2
    heads = lam_ref.shape[0]
    rows, depth = tok_ref.shape
    feats = q_ref.shape[1]
    part_rows = rows // CHUNKS
    partner = (1 - half) * place + pos
    beside = me + 1 - 2 * y
    other = dp + 1 - 2 * core

    def at_pos(p):
        return half * place + p

    ups = [(level + k) % levels for k in range(1, levels)]
    xs = [(x + k) % spans for k in range(1, spans)]
    in_half = [(pos + k) % place for k in range(1, place)]
    sp_peers = [(me + k) % n for k in range(1, n)]
    dp_peers = [(dp + k) % m for k in range(1, m)]
    done = []

    def lane(start, size):
        return pl.ds(pl.multiple_of(start, size), size)

    locals_ = [
        pltpu.make_async_copy(tok_ref, tokens.at[pos], local_sem.at[0]),
        pltpu.make_async_copy(cot_ref.at[:, lane(me * feats, feats)], coth.at[me], local_sem.at[1]),
    ] + [
        pltpu.make_async_copy(
            w_ref.at[:, lane((j * place + pos) * feats, feats)],
            wc.at[me, dp, :, pl.ds(j * feats, feats)],
            local_sem.at[2 + j],
        )
        for j in range(2)
    ]
    for copy in locals_:
        copy.start()
    greet([(s, dp) for s in sp_peers] + [(me, d) for d in dp_peers])

    def begin(copy):
        copy.start()
        done.append(copy)
        return copy

    wa = [
        begin(
            remote(
                w_ref.at[:, lane((j * place + p) * feats, feats)],
                wc.at[me, dp, :, pl.ds(j * feats, feats)],
                wa_s.at[k, j],
                wa_r.at[k, j],
                at_pos(p),
                dp,
            )
        )
        for k, p in enumerate(in_half)
        for j in range(2)
    ]

    def chunk(c):
        return pl.ds(c * part_rows, part_rows)

    def tok_up(k, c):
        return begin(
            remote(
                tok_ref.at[chunk(c)],
                tokens.at[pos, chunk(c)],
                tz_s.at[k, c],
                tz_r.at[k, c],
                at_pos(ups[k] * 2 + y),
                dp,
            )
        )

    def tok_own(c):
        return begin(
            remote(
                tok_ref.at[chunk(c)],
                tokens.at[pos, chunk(c)],
                ty_s.at[0, c],
                ty_r.at[0, c],
                beside,
                dp,
            )
        )

    def tok_side(k, c):
        origin = ((level + levels - k - 1) % levels) * 2 + y
        return begin(
            remote(
                tokens.at[origin, chunk(c)],
                tokens.at[origin, chunk(c)],
                ty_s.at[k + 1, c],
                ty_r.at[k + 1, c],
                beside,
                dp,
            )
        )

    up, own, side = {}, {}, {}
    early = CHUNKS // 2
    for c in range(early):
        for k in range(levels - 1):
            up[k, c] = tok_up(k, c)
        own[c] = tok_own(c)

    att = Attention(
        lam_ref, q_ref, k_ref, v_ref, coth,
        (p_ref, a_ref, qh_ref, kt_ref, go_ref, gv_acc, gk_acc),
        (gq_ref, gk_ref, gl_ref), width,
    )
    pieces = [(h, i) for h in range(heads) for i in range(att.count)]
    for h in range(heads):
        att.prepare(h)
    first = len(pieces) // 2
    for h, i in pieces[:first]:
        att.softmaxes(h, i)

    def wc_block(h, d):
        return wc.at[pl.ds(h * place, place), d]

    for copy in locals_[2:]:
        copy.wait()
    for copy in wa:
        copy.wait_recv()
    mine = wc_block(half, dp)
    wb = [begin(remote(mine, mine, wb_s.at[0], wb_r.at[0], partner, dp))]
    wx = [
        begin(remote(mine, mine, wx_s.at[0, k], wx_r.at[0, k], me, xk * 2 + core))
        for k, xk in enumerate(xs)
    ]
    wd = [begin(remote(mine, mine, wd_s.at[0], wd_r.at[0], me, other))]
    for c in range(early, CHUNKS):
        for k in range(levels - 1):
            up[k, c] = tok_up(k, c)
        own[c] = tok_own(c)
    for c in range(early):
        for k in range(levels - 1):
            up[k, c].wait_recv()
            side[k, c] = tok_side(k, c)
    for h, i in pieces[first:]:
        att.softmaxes(h, i)

    for k in range(spans - 1):
        origin = (x + spans - k - 1) % spans
        wx[k].wait_recv()
        block = wc_block(half, origin * 2 + core)
        wd.append(begin(remote(block, block, wd_s.at[1 + k], wd_r.at[1 + k], me, other)))
    for c in range(early, CHUNKS):
        for k in range(levels - 1):
            up[k, c].wait_recv()
            side[k, c] = tok_side(k, c)
    cots = [
        begin(
            remote(
                cot_ref.at[:, lane(s * feats, feats)],
                coth.at[me],
                c_s.at[k],
                c_r.at[k],
                s,
                dp,
            )
        )
        for k, s in enumerate(sp_peers)
    ]
    locals_[0].wait()

    def turn(b):
        tok_t[:, lane(b * rows, rows)] = tokens[b].astype(F32).T.astype(BF16)

    turn(pos)
    wb[0].wait_recv()
    block = wc_block(1 - half, dp)
    wx2 = [
        begin(remote(block, block, wx_s.at[1, k], wx_r.at[1, k], me, xk * 2 + core))
        for k, xk in enumerate(xs)
    ]
    wd.append(begin(remote(block, block, wd_s.at[spans], wd_r.at[spans], me, other)))
    for k in range(levels - 1):
        turn(((level + levels - k - 1) % levels) * 2 + y)
    for c in range(CHUNKS):
        own[c].wait_recv()
    turn(level * 2 + 1 - y)
    for k in range(spans - 1):
        origin = (x + spans - k - 1) % spans
        wx2[k].wait_recv()
        block = wc_block(1 - half, origin * 2 + core)
        slot = spans + 1 + k
        wd.append(begin(remote(block, block, wd_s.at[slot], wd_r.at[slot], me, other)))
    for copy in wd:
        copy.wait_recv()

    def weight():
        return wc[...].reshape(depth, 2 * feats)

    def values_of(b, k):
        vloc[b] = dot_nn(tokens[b], weight()).astype(BF16)
        copy = begin(
            remote(
                vloc.at[b, :, lane((1 - half) * feats, feats)],
                v_ref.at[half, b],
                v_s.at[k],
                v_r.at[k],
                partner,
                dp,
            )
        )
        v_ref[half, b] = vloc[b, :, lane(half * feats, feats)]
        return copy

    downs = [(level + levels - k - 1) % levels for k in range(levels - 1)]
    v_copies = [values_of(pos, 0)]
    for k in range(levels - 1):
        v_copies.append(values_of(downs[k] * 2 + y, 1 + k))
    v_copies.append(values_of(level * 2 + 1 - y, levels))
    for k in range(levels - 1):
        for c in range(CHUNKS):
            side[k, c].wait_recv()
        b = downs[k] * 2 + 1 - y
        v_copies.append(values_of(b, levels + 1 + k))
    for k in range(levels - 1):
        turn(downs[k] * 2 + 1 - y)
    for copy in v_copies:
        copy.wait_recv()
    locals_[1].wait()
    for copy in cots:
        copy.wait_recv()

    for h in range(heads):
        att.values_grad(h)
        gvb[:, :, :, h * width : (h + 1) * width] = (
            gv_acc[...].astype(BF16).reshape(2, place, rows, width)
        )
    order = (
        [u * 2 + 1 - y for u in ups] + [level * 2 + 1 - y] + [u * 2 + y for u in ups] + [pos]
    )
    dv_copies = [
        begin(
            remote(
                gvb.at[1 - half, b],
                dv.at[b, :, lane(half * feats, feats)],
                dv_s.at[k],
                dv_r.at[k],
                partner,
                dp,
            )
        )
        for k, b in enumerate(order)
    ]
    for b in range(place):
        dv[b, :, lane(half * feats, feats)] = gvb[half, b]
    split = (heads + 1) // 2
    for h in range(split):
        att.scores_grad(h)

    def partial(k):
        dv_copies[k].wait_recv()
        part[order[k]] = dot_nt(dv[order[k]], weight()).astype(BF16)

    ys = {}
    for k in range(levels):
        partial(k)
        slot = k if k < levels - 1 else levels - 1
        for c in range(CHUNKS):
            ys[k, c] = begin(
                remote(
                    part.at[order[k], chunk(c)],
                    ry.at[slot, chunk(c)],
                    y_s.at[slot, c],
                    y_r.at[slot, c],
                    beside,
                    dp,
                )
            )
    for h in range(split, heads):
        att.scores_grad(h)
    for k in range(levels, 2 * levels):
        partial(k)
    ls = [
        begin(remote(gl_ref, lbuf.at[k], l_s.at[k], l_r.at[k], me, d))
        for k, d in enumerate(dp_peers)
    ]

    count = w_ref.shape[0]
    stretch = m * count
    dv_all = dv[...].reshape(place * rows, 2 * feats)
    as_, bs, es, ds_ = {}, {}, {}, {}
    for p in range(place):
        for h in range(2):
            start = (h * place + p) * stretch
            term[h, p] = (
                dot_nn(tok_t[start : start + stretch], dv_all)
                .astype(BF16)
                .reshape(spans, 2, count, 2 * feats)
            )
        as_[p] = begin(
            remote(term.at[:, p, :, 1 - core], ra.at[p], a_s.at[p], a_r.at[p], me, other)
        )
    for p in range(place):
        as_[p].wait_recv()
        sa[p] = (term[:, p, :, core].astype(F32) + ra[p].astype(F32)).astype(BF16)
        for k, xk in enumerate(xs):
            bs[p, k] = begin(
                remote(
                    sa.at[p, :, xk], rb.at[k, p], b_s.at[k, p], b_r.at[k, p], me, xk * 2 + core
                )
            )

    def rows_up(c):
        for k in range(levels - 1):
            ys[k, c].wait_recv()
            total = part[ups[k] * 2 + y, chunk(c)].astype(F32) + ry[k, chunk(c)].astype(F32)
            sz[k, chunk(c)] = total.astype(BF16)
            zs[k, c] = begin(
                remote(
                    sz.at[k, chunk(c)],
                    rz.at[k, chunk(c)],
                    z_s.at[k, c],
                    z_r.at[k, c],
                    at_pos(ups[k] * 2 + y),
                    dp,
                )
            )

    def to_partner(p):
        total = sa[p, :, x].astype(F32)
        for k in range(spans - 1):
            bs[p, k].wait_recv()
            total = total + rb[k, p].astype(F32)
        sb[p] = total.astype(BF16)
        es[p] = begin(remote(sb.at[p, 1 - half], rc.at[p], e_s.at[p], e_r.at[p], partner, dp))

    def finish(p):
        es[p].wait_recv()
        sc[p] = (sb[p, half].astype(F32) + rc[p].astype(F32)).astype(BF16)

    zs = {}
    for i in range(max(place, CHUNKS)):
        if i < CHUNKS:
            rows_up(i)
        if i < place:
            to_partner(i)
        if 0 < i <= place:
            finish(i - 1)
    for i in range(max(place, CHUNKS) - 1, place):
        finish(i)
    for k, p in enumerate(in_half):
        ds_[k] = begin(
            remote(sc.at[p], rd.at[pos], d_s.at[k], d_r.at[k], at_pos(p), dp)
        )
    rd[pos] = sc[pos]
    for c in range(CHUNKS):
        total = part[pos, chunk(c)].astype(F32)
        ys[levels - 1, c].wait_recv()
        total = total + ry[levels - 1, chunk(c)].astype(F32)
        for k in range(levels - 1):
            zs[k, c].wait_recv()
            total = total + rz[k, chunk(c)].astype(F32)
        gt_ref[chunk(c)] = total.astype(BF16)
    lam = gl_ref[...]
    for k in range(m - 1):
        ls[k].wait_recv()
        lam = lam + lbuf[k]
    glo_ref[...] = lam
    for k in range(place - 1):
        ds_[k].wait_recv()
    for p in range(place):
        for j in range(2):
            start = (j * place + p) * feats
            gw_ref[:, start : start + feats] = rd[p, :, j * feats : (j + 1) * feats].astype(F32)
    for copy in done:
        copy.wait_send()


def run(lambdas, tokens, cotangent, weight, queries, keys, n, m, width):
    rows, depth = tokens.shape
    count, features = weight.shape
    length, feats = queries.shape
    heads = feats // width
    place, levels, spans = n // 2, n // 4, m // 2
    block = min(QBLOCK, length)
    blocks = length // block
    tri = block * (blocks * (blocks + 1) // 2)
    vmem = pl.BlockSpec(memory_space=pltpu.VMEM)
    hbm = pl.BlockSpec(memory_space=pltpu.HBM)
    pair = 2 * feats

    def b16(*shape):
        return pltpu.VMEM(shape, BF16)

    def f32(*shape):
        return pltpu.VMEM(shape, F32)

    def dma(*shape):
        return [pltpu.SemaphoreType.DMA(tuple(max(s, 1) for s in shape))] * 2

    return pl.pallas_call(
        functools.partial(whole_kernel, n, m, width),
        out_shape=[
            jax.ShapeDtypeStruct((length, feats), BF16),
            jax.ShapeDtypeStruct((length, feats), BF16),
            jax.ShapeDtypeStruct((rows, depth), BF16),
            jax.ShapeDtypeStruct((count, features), F32),
            jax.ShapeDtypeStruct((heads, 8, 128), F32),
        ],
        in_specs=[pl.BlockSpec(memory_space=pltpu.SMEM), hbm, hbm, hbm, vmem, vmem],
        out_specs=[vmem] * 5,
        scratch_shapes=[
            b16(place, rows, depth),
            b16(depth, place * rows),
            b16(n, m, count, pair),
            b16(n, rows, feats),
            b16(place, rows, pair),
            b16(2, place, rows, feats),
            f32(heads, 2, tri, block),
            b16(heads, tri, block),
            b16(heads, 2, length, width),
            b16(heads, 2, width, length),
            b16(heads, width, length),
            f32(length, width),
            f32(length, width),
            b16(2, place, rows, feats),
            b16(place, rows, pair),
            b16(place, rows, depth),
            b16(levels, rows, depth),
            b16(max(levels - 1, 1), rows, depth),
            b16(max(levels - 1, 1), rows, depth),
            b16(2, place, spans, 2, count, pair),
            b16(place, 2, spans, count, pair),
            b16(place, 2, spans, count, pair),
            b16(max(spans - 1, 1), place, 2, count, pair),
            b16(place, 2, count, pair),
            b16(place, count, pair),
            b16(place, count, pair),
            b16(place, count, pair),
            f32(heads, 8, 128),
            f32(m - 1, heads, 8, 128),
            pltpu.SemaphoreType.DMA((4,)),
        ]
        + dma(place - 1, 2)
        + dma(1)
        + dma(2, spans - 1)
        + dma(2 * spans)
        + dma(levels - 1, CHUNKS)
        + dma(levels, CHUNKS)
        + dma(n - 1)
        + dma(place)
        + dma(place)
        + dma(levels, CHUNKS)
        + dma(levels - 1, CHUNKS)
        + dma(place)
        + dma(spans - 1, place)
        + dma(place)
        + dma(place - 1)
        + dma(m - 1),
        compiler_params=pltpu.CompilerParams(
            collective_id=0, has_side_effects=True, vmem_limit_bytes=60 * 1024 * 1024
        ),
        name="whole",
    )(lambdas, tokens, cotangent, weight, queries, keys)


def body(n, m, tokens, cotangent, value_weight, query_heads, key_heads, lambdas):
    _, length, head_count, width = query_heads.shape
    feats = head_count * width
    grad_query, grad_key, grad_tokens, grad_weight, lambda_sum = run(
        lambdas,
        tokens[0],
        cotangent[0],
        value_weight,
        query_heads.reshape(length, feats),
        key_heads.reshape(length, feats),
        n,
        m,
        width,
    )
    return (
        grad_query.reshape(1, length, head_count, width),
        grad_key.reshape(1, length, head_count, width),
        grad_tokens[None],
        grad_weight,
        lambda_sum[:, 0, 0],
    )


def solution(mesh):
    placed = (
        P("dp", "sp", None),
        P("dp", "sp", None),
        P(("sp", "dp"), None),
        P("dp", None, "sp", None),
        P("dp", None, "sp", None),
        P("sp"),
    )
    return jax.shard_map(
        functools.partial(body, mesh.shape["sp"], mesh.shape["dp"]),
        mesh=mesh,
        in_specs=placed,
        out_specs=(
            P("dp", None, "sp", None),
            P("dp", None, "sp", None),
            P("dp", "sp", None),
            P(("sp", "dp"), None),
            P("sp"),
        ),
        check_vma=False,
    )
```

```python
import functools
import math

import jax
import jax.numpy as jnp
from jax import lax
from jax.experimental import pallas as pl
from jax.experimental.pallas import tpu as pltpu
from jax.sharding import PartitionSpec as P

QBLOCK = 256
EPS = 1e-06
NEGATIVE = -1e30
CHUNKS = 4
F32 = jnp.float32
BF16 = jnp.bfloat16


def dot_nn(a, b):
    return jnp.dot(a, b, preferred_element_type=F32)


def dot_nt(a, b):
    return lax.dot_general(a, b, (((1,), (1,)), ((), ())), preferred_element_type=F32)


def remote(src, dst, send, recv, sp, dp):
    return pltpu.make_async_remote_copy(
        src_ref=src,
        dst_ref=dst,
        send_sem=send,
        recv_sem=recv,
        device_id=(sp, dp),
        device_id_type=pl.DeviceIdType.MESH,
    )


def greet(peers):
    barrier = pltpu.get_barrier_semaphore()
    for sp, dp in peers:
        pl.semaphore_signal(
            barrier, inc=1, device_id=(sp, dp), device_id_type=pl.DeviceIdType.MESH
        )
    pl.semaphore_wait(barrier, len(peers))


class Attention:
    def __init__(self, lam_ref, q_ref, k_ref, v_ref, g_ref, bufs, outs, width):
        self.lam_ref, self.q_ref, self.k_ref = lam_ref, q_ref, k_ref
        self.v_ref, self.g_ref, self.width = v_ref, g_ref, width
        self.p_ref, self.a_ref, self.qh_ref, self.kt_ref, self.go_ref = bufs[:5]
        self.gv_acc, self.gk_acc = bufs[5:]
        self.gq_ref, self.gk_ref, self.gl_ref = outs
        self.length = q_ref.shape[0]
        self.block = min(QBLOCK, self.length)
        self.count = self.length // self.block

    def span(self, index):
        off = index * self.block
        reach = off + self.block
        pieces = ([(0, off)] if off else []) + [(off, reach)]
        base = self.block * (index * (index + 1) // 2)
        return off, reach, pieces, base

    def columns(self, head):
        return slice(head * self.width, (head + 1) * self.width)

    def prepare(self, head):
        length, width = self.length, self.width
        half = width // 2
        scaling = half ** (-0.5)
        lanes = lax.broadcasted_iota(jnp.int32, (length, width), 1)
        first_half = lanes < half
        q_all = self.q_ref[:, self.columns(head)].astype(F32) * scaling
        k_all = self.k_ref[:, self.columns(head)].astype(F32) * scaling
        self.qh_ref[head, 0] = jnp.where(first_half, q_all, 0.0).astype(BF16)
        self.qh_ref[head, 1] = jnp.where(first_half, 0.0, q_all).astype(BF16)
        self.kt_ref[head, 0] = jnp.where(first_half, k_all, 0.0).T.astype(BF16)
        self.kt_ref[head, 1] = jnp.where(first_half, 0.0, k_all).T.astype(BF16)

    def softmaxes(self, head, index):
        block = self.block
        lam = self.lam_ref[head]
        keep = lax.broadcasted_iota(jnp.int32, (block, block), 0) <= lax.broadcasted_iota(
            jnp.int32, (block, block), 1
        )
        off, reach, pieces, base = self.span(index)
        probs = []
        for c in range(2):
            qc = self.qh_ref[head, c, off:reach]
            scores = [dot_nt(self.k_ref[lo:hi, self.columns(head)], qc) for lo, hi in pieces]
            scores[-1] = jnp.where(keep, scores[-1], NEGATIVE)
            top = functools.reduce(
                jnp.maximum, [jnp.max(s, axis=0, keepdims=True) for s in scores]
            )
            exps = [jnp.exp(s - top) for s in scores]
            total = sum(jnp.sum(e, axis=0, keepdims=True) for e in exps)
            inv = 1.0 / total
            probs.append([e * inv for e in exps])
            for (lo, hi), p in zip(pieces, probs[c]):
                self.p_ref[head, c, base + lo : base + hi] = p
        for (lo, hi), p1, p2 in zip(pieces, *probs):
            self.a_ref[head, base + lo : base + hi] = (p1 - lam * p2).astype(BF16)

    def values_grad(self, head):
        width = self.width
        v_all = self.v_ref[:, :, :, self.columns(head)].reshape(self.length, width)
        vt = v_all.astype(F32).T.astype(BF16)
        gt = self.g_ref[:, :, self.columns(head)].reshape(self.length, width).astype(F32).T
        for index in range(self.count):
            off, reach, pieces, base = self.span(index)
            weights = self.a_ref[head, base : base + reach]
            out_t = dot_nn(vt[:, :reach], weights)
            cot = gt[:, off:reach]
            inverse = lax.rsqrt(jnp.mean(out_t * out_t, axis=0, keepdims=True) + EPS)
            normed = out_t * inverse
            grad_out = (
                inverse * (cot - normed * jnp.mean(cot * normed, axis=0, keepdims=True))
            ).astype(BF16)
            self.go_ref[head, :, off:reach] = grad_out
            gv = dot_nt(weights, grad_out)
            if off:
                self.gv_acc[0:off] += gv[0:off]
            self.gv_acc[off:reach] = gv[off:reach]

    def scores_grad(self, head):
        block, width = self.block, self.width
        lam = self.lam_ref[head]
        v_all = self.v_ref[:, :, :, self.columns(head)].reshape(self.length, width)
        lambda_total = jnp.zeros((1, block), F32)
        for index in range(self.count):
            off, reach, pieces, base = self.span(index)
            grad_out = self.go_ref[head, :, off:reach]
            probs = [
                [self.p_ref[head, c, base + lo : base + hi] for lo, hi in pieces]
                for c in range(2)
            ]
            grad_w = [dot_nn(v_all[lo:hi], grad_out) for lo, hi in pieces]
            sums = [
                sum(jnp.sum(d * p, axis=0, keepdims=True) for d, p in zip(grad_w, probs[c]))
                for c in range(2)
            ]
            lambda_total = lambda_total - sums[1]
            first = [(p * (d - sums[0])).astype(BF16) for d, p in zip(grad_w, probs[0])]
            second = [(-lam * p * (d - sums[1])).astype(BF16) for d, p in zip(grad_w, probs[1])]
            gq_t = sum(
                dot_nn(self.kt_ref[head, 0, :, lo:hi], a)
                + dot_nn(self.kt_ref[head, 1, :, lo:hi], b)
                for (lo, hi), a, b in zip(pieces, first, second)
            )
            self.gq_ref[off:reach, self.columns(head)] = gq_t.T.astype(BF16)
            for (lo, hi), a, b in zip(pieces, first, second):
                gk = dot_nn(a, self.qh_ref[head, 0, off:reach]) + dot_nn(
                    b, self.qh_ref[head, 1, off:reach]
                )
                if lo == off:
                    self.gk_acc[lo:hi, :] = gk
                else:
                    self.gk_acc[lo:hi, :] += gk
        self.gk_ref[:, self.columns(head)] = self.gk_acc[...].astype(BF16)
        self.gl_ref[head] = jnp.broadcast_to(
            jnp.sum(lambda_total, axis=1, keepdims=True), self.gl_ref.shape[1:]
        )


def whole_kernel(
    n, m,
    lam_in, tok_ref, cot_ref, w_ref, q_ref, k_ref,
    gq_ref, gk_ref, gt_ref, gw_ref, glo_ref,
    lam_ref, q_nat, k_nat, qf, kf, gqf, gkf,
    tokens, tok_t, wc, coth, vloc, v_ref, p_ref, a_ref, qh_ref, kt_ref, go_ref, gv_acc, gk_acc,
    gvb, dv, part, ry, sz, rz, term, ra, sa, rb, sb, rc, sc, rd, gl_ref, lbuf,
    local_sem, wa_s, wa_r, wx_s, wx_r, wd_s, wd_r, tz_s, tz_r, ty_s, ty_r,
    c_s, c_r, v_s, v_r, dv_s, dv_r, y_s, y_r, z_s, z_r, a_s, a_r, b_s, b_r, e_s, e_r,
    d_s, d_r, l_s, l_r,
):
    me = lax.axis_index("sp")
    dp = lax.axis_index("dp")
    place = n // 2
    levels = place // 2
    spans = m // 2
    half, pos = me // place, me % place
    level, y = pos // 2, pos % 2
    x, core = dp // 2, dp % 2
    rows, depth = tok_ref.shape
    length, heads, width = q_ref.shape
    feats = heads * width
    part_rows = rows // CHUNKS
    partner = (1 - half) * place + pos
    beside = me + 1 - 2 * y
    other = dp + 1 - 2 * core

    def at_pos(p):
        return half * place + p

    ups = [(level + k) % levels for k in range(1, levels)]
    xs = [(x + k) % spans for k in range(1, spans)]
    in_half = [(pos + k) % place for k in range(1, place)]
    sp_peers = [(me + k) % n for k in range(1, n)]
    dp_peers = [(dp + k) % m for k in range(1, m)]
    done = []

    def lane(start, size):
        return pl.ds(pl.multiple_of(start, size), size)

    locals_ = [
        pltpu.make_async_copy(tok_ref, tokens.at[pos], local_sem.at[0]),
        pltpu.make_async_copy(cot_ref.at[:, lane(me * feats, feats)], coth.at[me], local_sem.at[1]),
    ] + [
        pltpu.make_async_copy(
            w_ref.at[:, lane((j * place + pos) * feats, feats)],
            wc.at[me, dp, :, pl.ds(j * feats, feats)],
            local_sem.at[2 + j],
        )
        for j in range(2)
    ] + [
        pltpu.make_async_copy(q_ref, q_nat, local_sem.at[4]),
        pltpu.make_async_copy(k_ref, k_nat, local_sem.at[5]),
        pltpu.make_async_copy(lam_in, lam_ref, local_sem.at[6]),
    ]
    for copy in locals_:
        copy.start()
    greet([(s, dp) for s in sp_peers] + [(me, d) for d in dp_peers])

    def begin(copy):
        copy.start()
        done.append(copy)
        return copy

    def weight_out(k, s, j):
        start = (j * place + s % place) * feats
        return begin(
            remote(
                w_ref.at[:, lane(start, feats)],
                wc.at[me, dp, :, pl.ds(j * feats, feats)],
                wa_s.at[k, j],
                wa_r.at[k, j],
                s,
                dp,
            )
        )

    def chunk(c):
        return pl.ds(c * part_rows, part_rows)

    def tok_up(k, c):
        return begin(
            remote(
                tok_ref.at[chunk(c)],
                tokens.at[pos, chunk(c)],
                tz_s.at[k, c],
                tz_r.at[k, c],
                at_pos(ups[k] * 2 + y),
                dp,
            )
        )

    def tok_side(slot, origin, c):
        src = tok_ref.at[chunk(c)] if slot == 0 else tokens.at[origin, chunk(c)]
        return begin(
            remote(
                src,
                tokens.at[origin, chunk(c)],
                ty_s.at[slot, c],
                ty_r.at[slot, c],
                beside,
                dp,
            )
        )

    def cot_out(k, s):
        return remote(
            cot_ref.at[:, lane(s * feats, feats)], coth.at[me], c_s.at[k], c_r.at[k], s, dp
        )

    far = [(1 - half) * place + (pos + k) % place for k in range(place)]
    near = [at_pos(p) for p in in_half]
    wa = [weight_out(place + k, s, j) for k, s in enumerate(near) for j in range(2)]
    wb = [[weight_out(k, s, j) for j in range(2)] for k, s in enumerate(far)]
    up, side = {}, {}
    for c in range(CHUNKS):
        for k in range(levels - 1):
            up[k, c] = tok_up(k, c)
    own = [tok_side(0, pos, c) for c in range(CHUNKS)]
    far_cots = [cot_out(k, s) for k, s in enumerate(far)]
    near_cots = [cot_out(place + k, s) for k, s in enumerate(near)]
    done.extend(far_cots + near_cots)
    for copy in far_cots:
        copy.start()
    att = Attention(
        lam_ref, qf, kf, v_ref, coth,
        (p_ref, a_ref, qh_ref, kt_ref, go_ref, gv_acc, gk_acc),
        (gqf, gkf, gl_ref), width,
    )
    for copy in locals_[4:]:
        copy.wait()
    qf[...] = q_nat[...].reshape(length, feats)
    kf[...] = k_nat[...].reshape(length, feats)
    pieces = [(h, i) for h in range(heads) for i in range(att.count)]
    for h in range(heads):
        att.prepare(h)
    first = len(pieces) // 2
    for h, i in pieces[:first]:
        att.softmaxes(h, i)

    def wc_block(h, p, d):
        return wc.at[h * place + p, d]

    for copy in locals_[2:4]:
        copy.wait()
    for copy in wa:
        copy.wait_recv()
    wx, wd = {}, []

    def core_out(slot, p, block):
        wd.append(
            begin(remote(block, block, wd_s.at[slot, p], wd_r.at[slot, p], me, other))
        )

    def x_out(j, p, block):
        for k, xk in enumerate(xs):
            wx[j, k, p] = begin(
                remote(
                    block, block, wx_s.at[j, k, p], wx_r.at[j, k, p], me, xk * 2 + core
                )
            )

    for p in range(place):
        block = wc_block(half, p, dp)
        x_out(0, p, block)
        core_out(0, p, block)
    for h, i in pieces[first:]:
        att.softmaxes(h, i)
    downs = [(level + levels - k - 1) % levels for k in range(levels - 1)]
    x_downs = [(x + spans - k - 1) % spans for k in range(spans - 1)]

    def side_on(c):
        for k in range(levels - 1):
            up[k, c].wait_recv()
            side[k, c] = tok_side(k + 1, downs[k] * 2 + y, c)

    def turn(b):
        tok_t[:, lane(b * rows, rows)] = tokens[b].astype(F32).T.astype(BF16)

    def x_on(j, p):
        for k, origin in enumerate(x_downs):
            wx[j, k, p].wait_recv()
            slot = (1 + k) if j == 0 else (spans + 1 + k)
            h, q = (half, p) if j == 0 else (1 - half, (pos + place - p) % place)
            core_out(slot, p, wc_block(h, q, origin * 2 + core))

    for k in range(place):
        for copy in wb[k]:
            copy.wait_recv()
        block = wc_block(1 - half, (pos + place - k) % place, dp)
        x_out(1, k, block)
        core_out(spans, k, block)
    for p in range(place):
        x_on(0, p)
    locals_[0].wait()
    for c in range(CHUNKS):
        side_on(c)
        if c == 0:
            turn(pos)
    for copy in near_cots:
        copy.start()
    for k in range(levels - 1):
        turn(downs[k] * 2 + y)
    for copy in own:
        copy.wait_recv()
    turn(level * 2 + 1 - y)
    for p in range(place):
        x_on(1, p)
    for copy in wd:
        copy.wait_recv()

    def weight():
        return wc[...].reshape(depth, 2 * feats)

    def values_of(b, k):
        vloc[b] = dot_nn(tokens[b], weight()).astype(BF16)
        copy = begin(
            remote(
                vloc.at[b, :, lane((1 - half) * feats, feats)],
                v_ref.at[half, b],
                v_s.at[k],
                v_r.at[k],
                partner,
                dp,
            )
        )
        v_ref[half, b] = vloc[b, :, lane(half * feats, feats)]
        return copy

    v_copies = [values_of(pos, 0)]
    for k in range(levels - 1):
        v_copies.append(values_of(downs[k] * 2 + y, 1 + k))
    v_copies.append(values_of(level * 2 + 1 - y, levels))
    for k in range(levels - 1):
        for c in range(CHUNKS):
            side[k, c].wait_recv()
        v_copies.append(values_of(downs[k] * 2 + 1 - y, levels + 1 + k))

    for k in range(levels - 1):
        turn(downs[k] * 2 + 1 - y)
    for copy in v_copies:
        copy.wait_recv()
    locals_[1].wait()
    for copy in near_cots + far_cots:
        copy.wait_recv()

    order = (
        [u * 2 + 1 - y for u in ups] + [level * 2 + 1 - y] + [u * 2 + y for u in ups] + [pos]
    )
    dv_copies = {}
    for h in range(heads):
        att.values_grad(h)
        gvb[h] = gv_acc[...].astype(BF16).reshape(2, place, rows, width)
        for k, b in enumerate(order):
            dv_copies[h, k] = begin(
                remote(
                    gvb.at[h, 1 - half, b],
                    dv.at[b, :, lane(half * feats + h * width, width)],
                    dv_s.at[h, k],
                    dv_r.at[h, k],
                    partner,
                    dp,
                )
            )
        for b in range(place):
            dv[b, :, lane(half * feats + h * width, width)] = gvb[h, half, b]
    split = (heads + 1) // 2
    for h in range(split):
        att.scores_grad(h)

    def dv_wait(k):
        for h in range(heads):
            dv_copies[h, k].wait_recv()

    def partial(k):
        part[order[k]] = dot_nt(dv[order[k]], weight()).astype(BF16)

    ys, zs = {}, {}
    for k in range(levels):
        dv_wait(k)
        partial(k)
        for c in range(CHUNKS):
            ys[k, c] = begin(
                remote(
                    part.at[order[k], chunk(c)],
                    ry.at[k, chunk(c)],
                    y_s.at[k, c],
                    y_r.at[k, c],
                    beside,
                    dp,
                )
            )
    for h in range(split, heads):
        att.scores_grad(h)
    ls = [
        begin(remote(gl_ref, lbuf.at[k], l_s.at[k], l_r.at[k], me, d))
        for k, d in enumerate(dp_peers)
    ]
    for k in range(levels, 2 * levels):
        dv_wait(k)

    count = w_ref.shape[0]
    stretch = m * count
    dv_all = dv[...].reshape(place * rows, 2 * feats)
    as_, bs, es, ds_ = {}, {}, {}, {}
    turns = in_half + [pos]
    for k, p in enumerate(turns):
        for h in range(2):
            start = pl.multiple_of((h * place + p) * stretch, stretch)
            term[h, p] = (
                dot_nn(tok_t[pl.ds(start, stretch), :], dv_all)
                .astype(BF16)
                .reshape(spans, 2, count, 2 * feats)
            )
        as_[k] = begin(
            remote(term.at[:, p, :, 1 - core], ra.at[p], a_s.at[k], a_r.at[k], me, other)
        )
    for k in range(levels, 2 * levels):
        partial(k)
    for k, p in enumerate(turns):
        as_[k].wait_recv()
        sa[p] = (term[:, p, :, core].astype(F32) + ra[p].astype(F32)).astype(BF16)
        for j, xk in enumerate(xs):
            bs[k, j] = begin(
                remote(
                    sa.at[p, :, xk], rb.at[j, p], b_s.at[j, k], b_r.at[j, k], me, xk * 2 + core
                )
            )

    def rows_up(c):
        for k in range(levels - 1):
            ys[k, c].wait_recv()
            total = part[ups[k] * 2 + y, chunk(c)].astype(F32) + ry[k, chunk(c)].astype(F32)
            sz[k, chunk(c)] = total.astype(BF16)
            zs[k, c] = begin(
                remote(
                    sz.at[k, chunk(c)],
                    rz.at[k, chunk(c)],
                    z_s.at[k, c],
                    z_r.at[k, c],
                    at_pos(ups[k] * 2 + y),
                    dp,
                )
            )

    def to_partner(k):
        p = turns[k]
        total = sa[p, :, x].astype(F32)
        for j in range(spans - 1):
            bs[k, j].wait_recv()
            total = total + rb[j, p].astype(F32)
        sb[p] = total.astype(BF16)
        es[k] = begin(remote(sb.at[p, 1 - half], rc.at[p], e_s.at[k], e_r.at[k], partner, dp))

    def finish(k):
        p = turns[k]
        es[k].wait_recv()
        total = (sb[p, half].astype(F32) + rc[p].astype(F32)).astype(BF16)
        if k < place - 1:
            sc[p] = total
            ds_[k] = begin(
                remote(sc.at[p], rd.at[pos], d_s.at[k], d_r.at[k], at_pos(p), dp)
            )
        else:
            rd[pos] = total

    for c in range(CHUNKS):
        rows_up(c)
    gq_ref[...] = gqf[...].reshape(gq_ref.shape)
    gk_ref[...] = gkf[...].reshape(gk_ref.shape)
    for k in range(place):
        to_partner(k)
        if k > 0:
            finish(k - 1)
    finish(place - 1)
    for c in range(CHUNKS):
        total = part[pos, chunk(c)].astype(F32)
        ys[levels - 1, c].wait_recv()
        total = total + ry[levels - 1, chunk(c)].astype(F32)
        for k in range(levels - 1):
            zs[k, c].wait_recv()
            total = total + rz[k, chunk(c)].astype(F32)
        gt_ref[chunk(c)] = total.astype(BF16)
    lam = gl_ref[...]
    for k in range(m - 1):
        ls[k].wait_recv()
        lam = lam + lbuf[k]
    glo_ref[...] = lam
    for k in range(place - 1):
        ds_[k].wait_recv()
    for p in range(place):
        for j in range(2):
            start = (j * place + p) * feats
            gw_ref[:, start : start + feats] = rd[p, :, j * feats : (j + 1) * feats].astype(F32)
    for copy in done:
        copy.wait_send()


def finish_kernel(gq_ref, gk_ref, gt_ref, gw_ref, gl_ref, *refs):
    outs, lam_out, sems = refs[:4], refs[4], refs[5]
    copies = [
        pltpu.make_async_copy(src, dst, sems.at[i])
        for i, (src, dst) in enumerate(zip((gq_ref, gk_ref, gt_ref, gw_ref), outs))
    ]
    for copy in copies:
        copy.start()
    for h in range(gl_ref.shape[0]):
        lam_out[h] = jnp.max(gl_ref[h])
    for copy in copies:
        copy.wait()


def finish(gq, gk, gt, gw, gl):
    vmem = pl.BlockSpec(memory_space=pltpu.VMEM)
    hbm = pl.BlockSpec(memory_space=pltpu.HBM)
    results = [gq, gk, gt, gw]
    return pl.pallas_call(
        finish_kernel,
        out_shape=[jax.ShapeDtypeStruct(a.shape, a.dtype) for a in results]
        + [jax.ShapeDtypeStruct(gl.shape[:1], F32)],
        in_specs=[vmem] * 5,
        out_specs=[hbm] * 4 + [pl.BlockSpec(memory_space=pltpu.SMEM)],
        scratch_shapes=[pltpu.SemaphoreType.DMA((4,))],
        compiler_params=pltpu.CompilerParams(vmem_limit_bytes=2 * 1024 * 1024),
        name="finish",
    )(*results, gl)


def run(lambdas, tokens, cotangent, weight, queries, keys, n, m):
    rows, depth = tokens.shape
    count, features = weight.shape
    length, heads, width = queries.shape
    feats = heads * width
    place, levels, spans = n // 2, n // 4, m // 2
    block = min(QBLOCK, length)
    blocks = length // block
    tri = block * (blocks * (blocks + 1) // 2)
    vmem = pl.BlockSpec(memory_space=pltpu.VMEM)
    hbm = pl.BlockSpec(memory_space=pltpu.HBM)
    pair = 2 * feats

    def b16(*shape):
        return pltpu.VMEM(shape, BF16)

    def f32(*shape):
        return pltpu.VMEM(shape, F32)

    def dma(*shape):
        return [pltpu.SemaphoreType.DMA(tuple(max(s, 1) for s in shape))] * 2

    scratch = (
        [
            pltpu.SMEM((heads,), F32),
            b16(length, heads, width),
            b16(length, heads, width),
            b16(length, feats),
            b16(length, feats),
            b16(length, feats),
            b16(length, feats),
            b16(place, rows, depth),
            b16(depth, place * rows),
            b16(n, m, count, pair),
            b16(n, rows, feats),
            b16(place, rows, pair),
            b16(2, place, rows, feats),
            f32(heads, 2, tri, block),
            b16(heads, tri, block),
            b16(heads, 2, length, width),
            b16(heads, 2, width, length),
            b16(heads, width, length),
            f32(length, width),
            f32(length, width),
            b16(heads, 2, place, rows, width),
            b16(place, rows, pair),
            b16(place, rows, depth),
            b16(levels, rows, depth),
            b16(max(levels - 1, 1), rows, depth),
            b16(max(levels - 1, 1), rows, depth),
            b16(2, place, spans, 2, count, pair),
            b16(place, 2, spans, count, pair),
            b16(place, 2, spans, count, pair),
            b16(max(spans - 1, 1), place, 2, count, pair),
            b16(place, 2, count, pair),
            b16(place, count, pair),
            b16(place, count, pair),
            b16(place, count, pair),
            f32(heads, 8, 128),
            f32(m - 1, heads, 8, 128),
            pltpu.SemaphoreType.DMA((7,)),
        ]
        + dma(n - 1, 2)
        + dma(2, spans - 1, place)
        + dma(2 * spans, place)
        + dma(levels - 1, CHUNKS)
        + dma(levels, CHUNKS)
        + dma(n - 1)
        + dma(place)
        + dma(heads, place)
        + dma(levels, CHUNKS)
        + dma(levels - 1, CHUNKS)
        + dma(place)
        + dma(spans - 1, place)
        + dma(place)
        + dma(place - 1)
        + dma(m - 1)
    )
    held = sum(
        math.prod(ref.shape) * jnp.dtype(ref.dtype).itemsize
        for ref in scratch
        if ref.memory_space == pltpu.VMEM
    )
    return pl.pallas_call(
        functools.partial(whole_kernel, n, m),
        out_shape=[
            jax.ShapeDtypeStruct((length, heads, width), BF16),
            jax.ShapeDtypeStruct((length, heads, width), BF16),
            jax.ShapeDtypeStruct((rows, depth), BF16),
            jax.ShapeDtypeStruct((count, features), F32),
            jax.ShapeDtypeStruct((heads, 8, 128), F32),
        ],
        in_specs=[pl.BlockSpec(memory_space=pltpu.HBM if heads > 1 else pl.ANY), hbm, hbm, hbm, hbm, hbm],
        out_specs=[vmem] * 5,
        scratch_shapes=scratch,
        compiler_params=pltpu.CompilerParams(
            collective_id=0, has_side_effects=True, vmem_limit_bytes=held + 8 * 1024 * 1024
        ),
        name="whole",
    )(lambdas, tokens, cotangent, weight, queries, keys)


def body(n, m, tokens, cotangent, value_weight, query_heads, key_heads, lambdas):
    large = [tokens[0], cotangent[0], value_weight, query_heads[0], key_heads[0]]
    if lambdas.size > 1:
        large = [lambdas] + large
    large = [pltpu.with_memory_space_constraint(a, pltpu.HBM) for a in large]
    if lambdas.size == 1:
        large = [lambdas] + large
    results = run(*large, n, m)
    grad_query, grad_key, grad_tokens, grad_weight, grad_lambda = finish(*results)
    return grad_query[None], grad_key[None], grad_tokens[None], grad_weight, grad_lambda


def solution(mesh):
    placed = (
        P("dp", "sp", None),
        P("dp", "sp", None),
        P(("sp", "dp"), None),
        P("dp", None, "sp", None),
        P("dp", None, "sp", None),
        P("sp"),
    )
    return jax.shard_map(
        functools.partial(body, mesh.shape["sp"], mesh.shape["dp"]),
        mesh=mesh,
        in_specs=placed,
        out_specs=(
            P("dp", None, "sp", None),
            P("dp", None, "sp", None),
            P("dp", "sp", None),
            P(("sp", "dp"), None),
            P("sp"),
        ),
        check_vma=False,
    )
```

```python
import functools
import math

import jax
import jax.numpy as jnp
from jax import lax
from jax.experimental import pallas as pl
from jax.experimental.pallas import tpu as pltpu
from jax.sharding import PartitionSpec as P

QBLOCK = 256
EPS = 1e-06
NEGATIVE = -1e30
CHUNKS = 4
F32 = jnp.float32
BF16 = jnp.bfloat16


def dot_nn(a, b):
    return jnp.dot(a, b, preferred_element_type=F32)


def dot_nt(a, b):
    return lax.dot_general(a, b, (((1,), (1,)), ((), ())), preferred_element_type=F32)


def remote(src, dst, send, recv, sp, dp):
    return pltpu.make_async_remote_copy(
        src_ref=src,
        dst_ref=dst,
        send_sem=send,
        recv_sem=recv,
        device_id=(sp, dp),
        device_id_type=pl.DeviceIdType.MESH,
    )


def greet(peers, copies):
    barrier = pltpu.get_barrier_semaphore()
    for sp, dp in peers:
        pl.semaphore_signal(
            barrier, inc=1, device_id=(sp, dp), device_id_type=pl.DeviceIdType.MESH
        )
    for copy in copies:
        copy.start()
    pl.semaphore_wait(barrier, len(peers))


class Attention:
    def __init__(self, lam_ref, q_ref, k_ref, v_ref, g_ref, bufs, outs, width):
        self.lam_ref, self.q_ref, self.k_ref = lam_ref, q_ref, k_ref
        self.v_ref, self.g_ref, self.width = v_ref, g_ref, width
        self.p_ref, self.a_ref, self.qh_ref, self.kt_ref, self.go_ref = bufs[:5]
        self.gv_acc, self.gk_acc = bufs[5:]
        self.gq_ref, self.gk_ref, self.gl_ref = outs
        self.length = q_ref.shape[0]
        self.block = min(QBLOCK, self.length)
        self.count = self.length // self.block

    def span(self, index):
        off = index * self.block
        reach = off + self.block
        pieces = ([(0, off)] if off else []) + [(off, reach)]
        base = self.block * (index * (index + 1) // 2)
        return off, reach, pieces, base

    def columns(self, head):
        return slice(head * self.width, (head + 1) * self.width)

    def prepare(self, head):
        length, width = self.length, self.width
        half = width // 2
        scaling = half ** (-0.5)
        lanes = lax.broadcasted_iota(jnp.int32, (length, width), 1)
        first_half = lanes < half
        q_all = self.q_ref[:, self.columns(head)].astype(F32) * scaling
        k_all = self.k_ref[:, self.columns(head)].astype(F32) * scaling
        self.qh_ref[head, 0] = jnp.where(first_half, q_all, 0.0).astype(BF16)
        self.qh_ref[head, 1] = jnp.where(first_half, 0.0, q_all).astype(BF16)
        self.kt_ref[head, 0] = jnp.where(first_half, k_all, 0.0).T.astype(BF16)
        self.kt_ref[head, 1] = jnp.where(first_half, 0.0, k_all).T.astype(BF16)

    def softmaxes(self, head, index):
        block = self.block
        lam = self.lam_ref[head]
        keep = lax.broadcasted_iota(jnp.int32, (block, block), 0) <= lax.broadcasted_iota(
            jnp.int32, (block, block), 1
        )
        off, reach, pieces, base = self.span(index)
        probs = []
        for c in range(2):
            qc = self.qh_ref[head, c, off:reach]
            scores = [dot_nt(self.k_ref[lo:hi, self.columns(head)], qc) for lo, hi in pieces]
            scores[-1] = jnp.where(keep, scores[-1], NEGATIVE)
            top = functools.reduce(
                jnp.maximum, [jnp.max(s, axis=0, keepdims=True) for s in scores]
            )
            exps = [jnp.exp(s - top) for s in scores]
            total = sum(jnp.sum(e, axis=0, keepdims=True) for e in exps)
            inv = 1.0 / total
            probs.append([e * inv for e in exps])
            for (lo, hi), p in zip(pieces, probs[c]):
                self.p_ref[head, c, base + lo : base + hi] = p
        for (lo, hi), p1, p2 in zip(pieces, *probs):
            self.a_ref[head, base + lo : base + hi] = (p1 - lam * p2).astype(BF16)

    def values_grad(self, head):
        width = self.width
        v_all = self.v_ref[:, :, :, self.columns(head)].reshape(self.length, width)
        vt = v_all.astype(F32).T.astype(BF16)
        gt = self.g_ref[:, :, self.columns(head)].reshape(self.length, width).astype(F32).T
        for index in range(self.count):
            off, reach, pieces, base = self.span(index)
            weights = self.a_ref[head, base : base + reach]
            out_t = dot_nn(vt[:, :reach], weights)
            cot = gt[:, off:reach]
            inverse = lax.rsqrt(jnp.mean(out_t * out_t, axis=0, keepdims=True) + EPS)
            normed = out_t * inverse
            grad_out = (
                inverse * (cot - normed * jnp.mean(cot * normed, axis=0, keepdims=True))
            ).astype(BF16)
            self.go_ref[head, :, off:reach] = grad_out
            gv = dot_nt(weights, grad_out)
            if off:
                self.gv_acc[0:off] += gv[0:off]
            self.gv_acc[off:reach] = gv[off:reach]

    def scores_grad(self, head, midway=None):
        block, width = self.block, self.width
        lam = self.lam_ref[head]
        v_all = self.v_ref[:, :, :, self.columns(head)].reshape(self.length, width)
        lambda_total = jnp.zeros((1, block), F32)
        for index in range(self.count):
            if midway and index == self.count - 1:
                midway()
            off, reach, pieces, base = self.span(index)
            grad_out = self.go_ref[head, :, off:reach]
            probs = [
                [self.p_ref[head, c, base + lo : base + hi] for lo, hi in pieces]
                for c in range(2)
            ]
            grad_w = [dot_nn(v_all[lo:hi], grad_out) for lo, hi in pieces]
            sums = [
                sum(jnp.sum(d * p, axis=0, keepdims=True) for d, p in zip(grad_w, probs[c]))
                for c in range(2)
            ]
            lambda_total = lambda_total - sums[1]
            first = [(p * (d - sums[0])).astype(BF16) for d, p in zip(grad_w, probs[0])]
            second = [(-lam * p * (d - sums[1])).astype(BF16) for d, p in zip(grad_w, probs[1])]
            gq_t = sum(
                dot_nn(self.kt_ref[head, 0, :, lo:hi], a)
                + dot_nn(self.kt_ref[head, 1, :, lo:hi], b)
                for (lo, hi), a, b in zip(pieces, first, second)
            )
            self.gq_ref[off:reach, self.columns(head)] = gq_t.T.astype(BF16)
            for (lo, hi), a, b in zip(pieces, first, second):
                gk = dot_nn(a, self.qh_ref[head, 0, off:reach]) + dot_nn(
                    b, self.qh_ref[head, 1, off:reach]
                )
                if lo == off:
                    self.gk_acc[lo:hi, :] = gk
                else:
                    self.gk_acc[lo:hi, :] += gk
        self.gk_ref[:, self.columns(head)] = self.gk_acc[...].astype(BF16)
        self.gl_ref[head] = jnp.broadcast_to(
            jnp.sum(lambda_total, axis=1, keepdims=True), self.gl_ref.shape[1:]
        )


def whole_kernel(
    n, m,
    lam_in, tok_ref, cot_ref, w_ref, q_ref, k_ref,
    gq_ref, gk_ref, gt_ref, gw_ref, glo_ref,
    lam_ref, q_nat, k_nat, qf, kf, gqf, gkf,
    tokens, tok_t, wc, coth, vloc, v_ref, p_ref, a_ref, qh_ref, kt_ref, go_ref, gv_acc, gk_acc,
    gvb, dv, part, ry, sz, rz, rzd, tokx, acc, sb, rc, sc, rd, gl_ref, lbuf,
    local_sem, wa_s, wa_r, wx_s, wx_r, wd_s, wd_r, tz_s, tz_r, ty_s, ty_r,
    c_s, c_r, v_s, v_r, dv_s, dv_r, y_s, y_r, z_s, z_r, zd_s, zd_r, tx_s, tx_r, gx_s, gx_r, gd_s, gd_r, e_s, e_r,
    d_s, d_r, l_s, l_r,
):
    me = lax.axis_index("sp")
    dp = lax.axis_index("dp")
    place = n // 2
    levels = place // 2
    spans = m // 2
    half, pos = me // place, me % place
    level, y = pos // 2, pos % 2
    x, core = dp // 2, dp % 2
    rows, depth = tok_ref.shape
    length, heads, width = q_ref.shape
    feats = heads * width
    part_rows = rows // CHUNKS
    partner = (1 - half) * place + pos
    beside = me + 1 - 2 * y
    other = dp + 1 - 2 * core

    def at_pos(p):
        return half * place + p

    ups = [(level + k) % levels for k in range(1, levels)]
    xs = [(x + k) % spans for k in range(1, spans)]
    in_half = [(pos + k) % place for k in range(1, place)]
    sp_peers = [(me + k) % n for k in range(1, n)]
    dp_peers = [(dp + k) % m for k in range(1, m)]
    done = []

    def lane(start, size):
        return pl.ds(pl.multiple_of(start, size), size)

    locals_ = [
        pltpu.make_async_copy(tok_ref, tokens.at[pos], local_sem.at[0]),
        pltpu.make_async_copy(cot_ref.at[:, lane(me * feats, feats)], coth.at[me], local_sem.at[1]),
    ] + [
        pltpu.make_async_copy(
            w_ref.at[:, lane((j * place + pos) * feats, feats)],
            wc.at[me, dp, :, pl.ds(j * feats, feats)],
            local_sem.at[2 + j],
        )
        for j in range(2)
    ] + [
        pltpu.make_async_copy(q_ref, q_nat, local_sem.at[4]),
        pltpu.make_async_copy(k_ref, k_nat, local_sem.at[5]),
        pltpu.make_async_copy(lam_in, lam_ref, local_sem.at[6]),
    ]
    greet([(s, dp) for s in sp_peers] + [(me, d) for d in dp_peers], locals_)

    def begin(copy):
        copy.start()
        done.append(copy)
        return copy

    def weight_out(k, s, j):
        start = (j * place + s % place) * feats
        return begin(
            remote(
                w_ref.at[:, lane(start, feats)],
                wc.at[me, dp, :, pl.ds(j * feats, feats)],
                wa_s.at[k, j],
                wa_r.at[k, j],
                s,
                dp,
            )
        )

    def chunk(c):
        return pl.ds(c * part_rows, part_rows)

    def tok_up(k, c):
        return begin(
            remote(
                tok_ref.at[chunk(c)],
                tokens.at[pos, chunk(c)],
                tz_s.at[k, c],
                tz_r.at[k, c],
                at_pos(ups[k] * 2 + y),
                dp,
            )
        )

    def tok_side(slot, origin, c):
        src = tok_ref.at[chunk(c)] if slot == 0 else tokens.at[origin, chunk(c)]
        return begin(
            remote(
                src,
                tokens.at[origin, chunk(c)],
                ty_s.at[slot, c],
                ty_r.at[slot, c],
                beside,
                dp,
            )
        )

    def cot_out(k, s):
        return remote(
            cot_ref.at[:, lane(s * feats, feats)], coth.at[me], c_s.at[k], c_r.at[me], s, dp
        )

    def cot_in(s):
        return remote(coth.at[s], coth.at[s], c_s.at[0], c_r.at[s], s, dp)

    far = [(1 - half) * place + (pos + k) % place for k in range(place)]
    near = [at_pos(p) for p in in_half]
    wa = [weight_out(place + k, s, j) for k, s in enumerate(near) for j in range(2)]
    wb = [[weight_out(k, s, j) for j in range(2)] for k, s in enumerate(far)]
    up, side = {}, {}
    for c in range(CHUNKS):
        for k in range(levels - 1):
            up[k, c] = tok_up(k, c)
    own = [tok_side(0, pos, c) for c in range(CHUNKS)]
    far_cots = [
        cot_out(
            2 * j + i,
            (1 - half) * place
            + (j + half * (levels - 1 - 2 * j)) * 2
            + (y if i == 0 else 1 - y),
        )
        for j in range(levels)
        for i in range(2)
    ]
    near_cots = [cot_out(place + k, s) for k, s in enumerate(near)]
    done.extend(far_cots + near_cots)
    for copy in far_cots:
        copy.start()
    att = Attention(
        lam_ref, qf, kf, v_ref, coth,
        (p_ref, a_ref, qh_ref, kt_ref, go_ref, gv_acc, gk_acc),
        (gqf, gkf, gl_ref), width,
    )
    for copy in locals_[4:]:
        copy.wait()
    qf[...] = q_nat[...].reshape(length, feats)
    kf[...] = k_nat[...].reshape(length, feats)
    pieces = [(h, i) for h in range(heads) for i in range(att.count)]
    for h in range(heads):
        att.prepare(h)
    first = len(pieces) // 2
    for h, i in pieces[:first]:
        att.softmaxes(h, i)

    def wc_block(h, p, d):
        return wc.at[h * place + p, d]

    for copy in locals_[2:4]:
        copy.wait()
    for copy in wa:
        copy.wait_recv()
    wx, wd = {}, []

    def core_out(slot, p, block):
        wd.append(
            begin(remote(block, block, wd_s.at[slot, p], wd_r.at[slot, p], me, other))
        )

    def x_out(j, p, block):
        for k, xk in enumerate(xs):
            wx[j, k, p] = begin(
                remote(
                    block, block, wx_s.at[j, k, p], wx_r.at[j, k, p], me, xk * 2 + core
                )
            )

    for p in range(place):
        block = wc_block(half, p, dp)
        x_out(0, p, block)
        core_out(0, p, block)
    for h, i in pieces[first:]:
        att.softmaxes(h, i)
    downs = [(level + levels - k - 1) % levels for k in range(levels - 1)]
    x_downs = [(x + spans - k - 1) % spans for k in range(spans - 1)]

    def side_on(c):
        for k in range(levels - 1):
            up[k, c].wait_recv()
            side[k, c] = tok_side(k + 1, downs[k] * 2 + y, c)

    count = w_ref.shape[0]
    txs = {}

    def turn(slot, b):
        turned = tokens[b].astype(F32).T.astype(BF16).reshape(2, place, m, count, rows)
        for h in range(2):
            for p in range(place):
                tok_t[b, p, h] = turned[h, p]
        stretch = lane((dp * place + b) * rows, rows)
        for k, d in enumerate(dp_peers):
            txs[k, slot] = begin(
                remote(
                    tok_t.at[b, :, :, d],
                    tokx.at[:, :, :, stretch],
                    tx_s.at[k, slot],
                    tx_r.at[k, slot],
                    me,
                    d,
                )
            )
        tokx[:, :, :, stretch] = tok_t[b, :, :, dp]

    def x_on(j, p):
        for k, origin in enumerate(x_downs):
            wx[j, k, p].wait_recv()
            slot = (1 + k) if j == 0 else (spans + 1 + k)
            h, q = (half, p) if j == 0 else (1 - half, (pos + place - p) % place)
            core_out(slot, p, wc_block(h, q, origin * 2 + core))

    for k in range(place):
        for copy in wb[k]:
            copy.wait_recv()
        block = wc_block(1 - half, (pos + place - k) % place, dp)
        x_out(1, k, block)
        core_out(spans, k, block)
    for p in range(place):
        x_on(0, p)
    locals_[0].wait()
    for c in range(CHUNKS):
        side_on(c)
        if c == 0:
            turn(0, pos)
        if c == CHUNKS // 2 - 1:
            for p in range(place):
                x_on(1, p)
    for copy in near_cots:
        copy.start()
    for k in range(levels - 1):
        turn(1 + k, downs[k] * 2 + y)
    for copy in own:
        copy.wait_recv()
    turn(levels, level * 2 + 1 - y)
    for copy in wd:
        copy.wait_recv()

    def weight():
        return wc[...].reshape(depth, 2 * feats)

    def values_of(b, k):
        vloc[b] = dot_nn(tokens[b], weight()).astype(BF16)
        copy = begin(
            remote(
                vloc.at[b, :, lane((1 - half) * feats, feats)],
                v_ref.at[half, b],
                v_s.at[k],
                v_r.at[k],
                partner,
                dp,
            )
        )
        v_ref[half, b] = vloc[b, :, lane(half * feats, feats)]
        return copy

    v_copies = [values_of(pos, 0)]
    for k in range(levels - 1):
        v_copies.append(values_of(downs[k] * 2 + y, 1 + k))
    v_copies.append(values_of(level * 2 + 1 - y, levels))
    for k in range(levels - 1):
        for c in range(CHUNKS):
            side[k, c].wait_recv()
        v_copies.append(values_of(downs[k] * 2 + 1 - y, levels + 1 + k))

    for k in range(levels - 1):
        turn(levels + 1 + k, downs[k] * 2 + 1 - y)
    for copy in v_copies:
        copy.wait_recv()
    locals_[1].wait()
    for s in sp_peers:
        cot_in(s).wait_recv()

    order = (
        [u * 2 + 1 - y for u in ups] + [level * 2 + 1 - y] + [u * 2 + y for u in ups] + [pos]
    )
    dv_copies = {}

    def dv_out(h, k):
        dv_copies[h, k] = begin(
            remote(
                gvb.at[h, 1 - half, order[k]],
                dv.at[dp, order[k], :, lane(half * feats + h * width, width)],
                dv_s.at[h, k],
                dv_r.at[h, k],
                partner,
                dp,
            )
        )

    for h in range(heads):
        att.values_grad(h)
        gvb[h] = gv_acc[...].astype(BF16).reshape(2, place, rows, width)
        dv_out(h, 0)
        for b in range(place):
            dv[dp, b, :, lane(half * feats + h * width, width)] = gvb[h, half, b]

    gxs, gds = {}, []

    def share(d, j):
        if j == 0:
            return dv.at[d, :, :, lane(half * feats, feats)]
        return dv.at[d, order[j - 1], :, lane((1 - half) * feats, feats)]

    def share_core(slot, j, d):
        gds.append(
            begin(
                remote(
                    share(d, j), share(d, j), gd_s.at[slot, j], gd_r.at[slot, j], me, other
                )
            )
        )

    def share_out(j):
        for k, xk in enumerate(xs):
            gxs[k, j] = begin(
                remote(
                    share(dp, j),
                    share(dp, j),
                    gx_s.at[k, j],
                    gx_r.at[k, j],
                    me,
                    xk * 2 + core,
                )
            )
        share_core(0, j, dp)

    def share_on(j):
        for k, origin in enumerate(x_downs):
            gxs[k, j].wait_recv()
            share_core(1 + k, j, origin * 2 + core)

    share_out(0)
    split = (heads + 1) // 2

    def dv_more():
        for h in range(heads):
            for k in range(1, levels):
                dv_out(h, k)

    for h in range(split):
        att.scores_grad(h, dv_more if h == 0 else None)

    def dv_wait(k):
        for h in range(heads):
            dv_copies[h, k].wait_recv()
        share_out(1 + k)

    def partial(k):
        part[order[k]] = dot_nt(dv[dp, order[k]], weight()).astype(BF16)

    ys, zs, zd = {}, {}, {}
    last = CHUNKS - 1

    def y_out(k, c):
        ys[k, c] = begin(
            remote(
                part.at[order[k], chunk(c)],
                ry.at[k, chunk(c)],
                y_s.at[k, c],
                y_r.at[k, c],
                beside,
                dp,
            )
        )

    for k in range(levels):
        dv_wait(k)
        if k == 0:
            for h in range(heads):
                for j in range(levels, 2 * levels):
                    dv_out(h, j)
        partial(k)
        for c in range(last):
            y_out(k, c)
        if k < levels - 1:
            zd[k] = begin(
                remote(
                    part.at[order[k], chunk(last)],
                    rzd.at[k],
                    zd_s.at[k],
                    zd_r.at[k],
                    at_pos(ups[k] * 2 + y),
                    dp,
                )
            )
    for h in range(split, heads):
        att.scores_grad(h)
    ls = [
        begin(remote(gl_ref, lbuf.at[k], l_s.at[k], l_r.at[k], me, d))
        for k, d in enumerate(dp_peers)
    ]
    def last_out():
        total = part[order[levels - 1], chunk(last)].astype(F32)
        for k in range(levels - 1):
            zd[k].wait_recv()
            total = total + rzd[k].astype(F32)
        part[order[levels - 1], chunk(last)] = total.astype(BF16)
        y_out(levels - 1, last)

    def rows_up(c):
        for k in range(levels - 1):
            total = part[ups[k] * 2 + y, chunk(c)].astype(F32)
            if c < last:
                ys[k, c].wait_recv()
                total = total + ry[k, chunk(c)].astype(F32)
            sz[k, chunk(c)] = total.astype(BF16)
            zs[k, c] = begin(
                remote(
                    sz.at[k, chunk(c)],
                    rz.at[k, chunk(c)],
                    z_s.at[k, c],
                    z_r.at[k, c],
                    at_pos(ups[k] * 2 + y),
                    dp,
                )
            )

    for k in range(levels, 2 * levels - 1):
        dv_wait(k)
        partial(k)
    rows_up(last)
    rows_up(0)
    last_out()
    dv_wait(2 * levels - 1)
    for j in range(place):
        share_on(j)
    for c in range(1, last - 1):
        rows_up(c)
    share_on(place)
    for k in range(m - 1):
        for slot in range(place):
            txs[k, slot].wait_recv()
    for copy in gds:
        copy.wait_recv()

    es, ds_ = {}, {}
    turns = in_half + [pos]
    dv_all = dv[...].reshape(m * place * rows, 2 * feats)
    for k, p in enumerate(turns):
        acc[p] = dot_nn(tokx[p].reshape(2 * count, m * place * rows), dv_all).reshape(
            2, count, 2 * feats
        )
        sb[p] = acc[p, 1 - half].astype(BF16)
        es[k] = begin(remote(sb.at[p], rc.at[p], e_s.at[k], e_r.at[k], partner, dp))
    rows_up(last - 1)
    partial(2 * levels - 1)

    def finish(k):
        p = turns[k]
        es[k].wait_recv()
        total = (acc[p, half] + rc[p].astype(F32)).astype(BF16)
        if k < place - 1:
            sc[p] = total
            ds_[k] = begin(
                remote(sc.at[p], rd.at[pos], d_s.at[k], d_r.at[k], at_pos(p), dp)
            )
        else:
            rd[pos] = total

    gq_ref[...] = gqf[...].reshape(gq_ref.shape)
    gk_ref[...] = gkf[...].reshape(gk_ref.shape)
    for k in range(place):
        finish(k)
    for c in range(CHUNKS):
        total = part[pos, chunk(c)].astype(F32)
        ys[levels - 1, c].wait_recv()
        total = total + ry[levels - 1, chunk(c)].astype(F32)
        for k in range(levels - 1):
            zs[k, c].wait_recv()
            total = total + rz[k, chunk(c)].astype(F32)
        gt_ref[chunk(c)] = total.astype(BF16)
    lam = gl_ref[...]
    for k in range(m - 1):
        ls[k].wait_recv()
        lam = lam + lbuf[k]
    glo_ref[...] = lam
    for k in range(place - 1):
        ds_[k].wait_recv()
    for p in range(place):
        for j in range(2):
            start = (j * place + p) * feats
            gw_ref[:, start : start + feats] = rd[p, :, j * feats : (j + 1) * feats].astype(F32)
    for copy in done:
        copy.wait_send()


def finish_kernel(gq_ref, gk_ref, gt_ref, gw_ref, gl_ref, *refs):
    outs, lam_out, sems = refs[:4], refs[4], refs[5]
    copies = [
        pltpu.make_async_copy(src, dst, sems.at[i])
        for i, (src, dst) in enumerate(zip((gq_ref, gk_ref, gt_ref, gw_ref), outs))
    ]
    for copy in copies:
        copy.start()
    for h in range(gl_ref.shape[0]):
        lam_out[h] = jnp.max(gl_ref[h])
    for copy in copies:
        copy.wait()


def finish(gq, gk, gt, gw, gl):
    vmem = pl.BlockSpec(memory_space=pltpu.VMEM)
    hbm = pl.BlockSpec(memory_space=pltpu.HBM)
    results = [gq, gk, gt, gw]
    return pl.pallas_call(
        finish_kernel,
        out_shape=[jax.ShapeDtypeStruct(a.shape, a.dtype) for a in results]
        + [jax.ShapeDtypeStruct(gl.shape[:1], F32)],
        in_specs=[vmem] * 5,
        out_specs=[hbm] * 4 + [pl.BlockSpec(memory_space=pltpu.SMEM)],
        scratch_shapes=[pltpu.SemaphoreType.DMA((4,))],
        compiler_params=pltpu.CompilerParams(vmem_limit_bytes=2 * 1024 * 1024),
        name="finish",
    )(*results, gl)


def run(lambdas, tokens, cotangent, weight, queries, keys, n, m):
    rows, depth = tokens.shape
    count, features = weight.shape
    length, heads, width = queries.shape
    feats = heads * width
    place, levels, spans = n // 2, n // 4, m // 2
    block = min(QBLOCK, length)
    blocks = length // block
    tri = block * (blocks * (blocks + 1) // 2)
    vmem = pl.BlockSpec(memory_space=pltpu.VMEM)
    hbm = pl.BlockSpec(memory_space=pltpu.HBM)
    pair = 2 * feats

    def b16(*shape):
        return pltpu.VMEM(shape, BF16)

    def f32(*shape):
        return pltpu.VMEM(shape, F32)

    def dma(*shape):
        return [pltpu.SemaphoreType.DMA(tuple(max(s, 1) for s in shape))] * 2

    scratch = (
        [
            pltpu.SMEM((heads,), F32),
            b16(length, heads, width),
            b16(length, heads, width),
            b16(length, feats),
            b16(length, feats),
            b16(length, feats),
            b16(length, feats),
            b16(place, rows, depth),
            b16(place, place, 2, m, count, rows),
            b16(n, m, count, pair),
            b16(n, rows, feats),
            b16(place, rows, pair),
            b16(2, place, rows, feats),
            f32(heads, 2, tri, block),
            b16(heads, tri, block),
            b16(heads, 2, length, width),
            b16(heads, 2, width, length),
            b16(heads, width, length),
            f32(length, width),
            f32(length, width),
            b16(heads, 2, place, rows, width),
            b16(m, place, rows, pair),
            b16(place, rows, depth),
            b16(levels, rows, depth),
            b16(max(levels - 1, 1), rows, depth),
            b16(max(levels - 1, 1), rows, depth),
            b16(max(levels - 1, 1), rows // CHUNKS, depth),
            b16(place, 2, count, m * place * rows),
            f32(place, 2, count, pair),
            b16(place, count, pair),
            b16(place, count, pair),
            b16(place, count, pair),
            b16(place, count, pair),
            f32(heads, 8, 128),
            f32(m - 1, heads, 8, 128),
            pltpu.SemaphoreType.DMA((7,)),
        ]
        + dma(n - 1, 2)
        + dma(2, spans - 1, place)
        + dma(2 * spans, place)
        + dma(levels - 1, CHUNKS)
        + dma(levels, CHUNKS)
        + dma(n)
        + dma(place)
        + dma(heads, place)
        + dma(levels, CHUNKS)
        + dma(levels - 1, CHUNKS)
        + dma(levels - 1)
        + dma(m - 1, place)
        + dma(spans - 1, place + 1)
        + dma(spans, place + 1)
        + dma(place)
        + dma(place - 1)
        + dma(m - 1)
    )
    held = sum(
        math.prod(ref.shape) * jnp.dtype(ref.dtype).itemsize
        for ref in scratch
        if ref.memory_space == pltpu.VMEM
    )
    return pl.pallas_call(
        functools.partial(whole_kernel, n, m),
        out_shape=[
            jax.ShapeDtypeStruct((length, heads, width), BF16),
            jax.ShapeDtypeStruct((length, heads, width), BF16),
            jax.ShapeDtypeStruct((rows, depth), BF16),
            jax.ShapeDtypeStruct((count, features), F32),
            jax.ShapeDtypeStruct((heads, 8, 128), F32),
        ],
        in_specs=[pl.BlockSpec(memory_space=pltpu.HBM if heads > 1 else pl.ANY), hbm, hbm, hbm, hbm, hbm],
        out_specs=[vmem] * 5,
        scratch_shapes=scratch,
        compiler_params=pltpu.CompilerParams(
            collective_id=0, has_side_effects=True, vmem_limit_bytes=held + 8 * 1024 * 1024
        ),
        name="whole",
    )(lambdas, tokens, cotangent, weight, queries, keys)


def body(n, m, tokens, cotangent, value_weight, query_heads, key_heads, lambdas):
    large = [tokens[0], cotangent[0], value_weight, query_heads[0], key_heads[0]]
    if lambdas.size > 1:
        large = [lambdas] + large
    large = [pltpu.with_memory_space_constraint(a, pltpu.HBM) for a in large]
    if lambdas.size == 1:
        large = [lambdas] + large
    results = run(*large, n, m)
    grad_query, grad_key, grad_tokens, grad_weight, grad_lambda = finish(*results)
    return grad_query[None], grad_key[None], grad_tokens[None], grad_weight, grad_lambda


def solution(mesh):
    placed = (
        P("dp", "sp", None),
        P("dp", "sp", None),
        P(("sp", "dp"), None),
        P("dp", None, "sp", None),
        P("dp", None, "sp", None),
        P("sp"),
    )
    return jax.shard_map(
        functools.partial(body, mesh.shape["sp"], mesh.shape["dp"]),
        mesh=mesh,
        in_specs=placed,
        out_specs=(
            P("dp", None, "sp", None),
            P("dp", None, "sp", None),
            P("dp", "sp", None),
            P(("sp", "dp"), None),
            P("sp"),
        ),
        check_vma=False,
    )
```

```python
import functools
import math

import jax
import jax.numpy as jnp
from jax import lax
from jax.experimental import pallas as pl
from jax.experimental.pallas import tpu as pltpu
from jax.sharding import PartitionSpec as P

QBLOCK = 256
EPS = 1e-06
NEGATIVE = -1e30
CHUNKS = 4
F32 = jnp.float32
BF16 = jnp.bfloat16


def dot_nn(a, b):
    return jnp.dot(a, b, preferred_element_type=F32)


def dot_nt(a, b):
    return lax.dot_general(a, b, (((1,), (1,)), ((), ())), preferred_element_type=F32)


def remote(src, dst, send, recv, sp, dp):
    return pltpu.make_async_remote_copy(
        src_ref=src,
        dst_ref=dst,
        send_sem=send,
        recv_sem=recv,
        device_id=(sp, dp),
        device_id_type=pl.DeviceIdType.MESH,
    )


def greet(peers, copies):
    barrier = pltpu.get_barrier_semaphore()
    for sp, dp in peers:
        pl.semaphore_signal(
            barrier, inc=1, device_id=(sp, dp), device_id_type=pl.DeviceIdType.MESH
        )
    for copy in copies:
        copy.start()
    pl.semaphore_wait(barrier, len(peers))


class Attention:
    def __init__(self, lam_ref, q_ref, k_ref, v_ref, g_ref, bufs, outs, width):
        self.lam_ref, self.q_ref, self.k_ref = lam_ref, q_ref, k_ref
        self.v_ref, self.g_ref, self.width = v_ref, g_ref, width
        self.p_ref, self.a_ref, self.qh_ref, self.kt_ref, self.go_ref = bufs[:5]
        self.gv_acc, self.gk_acc, self.vt_ref, self.gt_ref = bufs[5:]
        self.gq_ref, self.gk_ref, self.gl_ref = outs
        self.length = q_ref.shape[0]
        self.block = min(QBLOCK, self.length)
        self.count = self.length // self.block

    def span(self, index):
        off = index * self.block
        reach = off + self.block
        pieces = ([(0, off)] if off else []) + [(off, reach)]
        base = self.block * (index * (index + 1) // 2)
        return off, reach, pieces, base

    def columns(self, head):
        return slice(head * self.width, (head + 1) * self.width)

    def prepare(self, head):
        length, width = self.length, self.width
        half = width // 2
        scaling = half ** (-0.5)
        lanes = lax.broadcasted_iota(jnp.int32, (length, width), 1)
        first_half = lanes < half
        q_all = self.q_ref[:, self.columns(head)].astype(F32) * scaling
        k_all = self.k_ref[:, self.columns(head)].astype(F32) * scaling
        self.qh_ref[head, 0] = jnp.where(first_half, q_all, 0.0).astype(BF16)
        self.qh_ref[head, 1] = jnp.where(first_half, 0.0, q_all).astype(BF16)
        self.kt_ref[head, 0] = jnp.where(first_half, k_all, 0.0).T.astype(BF16)
        self.kt_ref[head, 1] = jnp.where(first_half, 0.0, k_all).T.astype(BF16)

    def softmaxes(self, head, index):
        block = self.block
        lam = self.lam_ref[head]
        keep = lax.broadcasted_iota(jnp.int32, (block, block), 0) <= lax.broadcasted_iota(
            jnp.int32, (block, block), 1
        )
        off, reach, pieces, base = self.span(index)
        probs = []
        for c in range(2):
            qc = self.qh_ref[head, c, off:reach]
            scores = [dot_nt(self.k_ref[lo:hi, self.columns(head)], qc) for lo, hi in pieces]
            scores[-1] = jnp.where(keep, scores[-1], NEGATIVE)
            top = functools.reduce(
                jnp.maximum, [jnp.max(s, axis=0, keepdims=True) for s in scores]
            )
            exps = [jnp.exp(s - top) for s in scores]
            total = sum(jnp.sum(e, axis=0, keepdims=True) for e in exps)
            inv = 1.0 / total
            probs.append([e * inv for e in exps])
            for (lo, hi), p in zip(pieces, probs[c]):
                self.p_ref[head, c, base + lo : base + hi] = p
        for (lo, hi), p1, p2 in zip(pieces, *probs):
            self.a_ref[head, base + lo : base + hi] = (p1 - lam * p2).astype(BF16)

    def turn_cotangent(self, head):
        wide = self.g_ref[:, :, self.columns(head)].reshape(self.length, self.width)
        self.gt_ref[head] = wide.astype(F32).T

    def turn_values(self, head, half):
        size = self.length // 2
        span = pl.ds(pl.multiple_of(half * size, size), size)
        values = self.v_ref[half, :, :, self.columns(head)].reshape(size, self.width)
        self.vt_ref[head, :, span] = values.astype(F32).T.astype(BF16)

    def values_grad(self, head):
        for index in range(self.count):
            off, reach, pieces, base = self.span(index)
            weights = self.a_ref[head, base : base + reach]
            out_t = dot_nn(self.vt_ref[head, :, :reach], weights)
            cot = self.gt_ref[head, :, off:reach]
            inverse = lax.rsqrt(jnp.mean(out_t * out_t, axis=0, keepdims=True) + EPS)
            normed = out_t * inverse
            grad_out = (
                inverse * (cot - normed * jnp.mean(cot * normed, axis=0, keepdims=True))
            ).astype(BF16)
            self.go_ref[head, :, off:reach] = grad_out
            gv = dot_nt(weights, grad_out)
            if off:
                self.gv_acc[0:off] += gv[0:off]
            self.gv_acc[off:reach] = gv[off:reach]

    def scores_grad(self, head, midway=None):
        block, width = self.block, self.width
        lam = self.lam_ref[head]
        v_all = self.v_ref[:, :, :, self.columns(head)].reshape(self.length, width)
        lambda_total = jnp.zeros((1, block), F32)
        for index in range(self.count):
            if midway and index == self.count - 1:
                midway()
            off, reach, pieces, base = self.span(index)
            grad_out = self.go_ref[head, :, off:reach]
            probs = [
                [self.p_ref[head, c, base + lo : base + hi] for lo, hi in pieces]
                for c in range(2)
            ]
            grad_w = [dot_nn(v_all[lo:hi], grad_out) for lo, hi in pieces]
            sums = [
                sum(jnp.sum(d * p, axis=0, keepdims=True) for d, p in zip(grad_w, probs[c]))
                for c in range(2)
            ]
            lambda_total = lambda_total - sums[1]
            first = [(p * (d - sums[0])).astype(BF16) for d, p in zip(grad_w, probs[0])]
            second = [(-lam * p * (d - sums[1])).astype(BF16) for d, p in zip(grad_w, probs[1])]
            gq_t = sum(
                dot_nn(self.kt_ref[head, 0, :, lo:hi], a)
                + dot_nn(self.kt_ref[head, 1, :, lo:hi], b)
                for (lo, hi), a, b in zip(pieces, first, second)
            )
            self.gq_ref[off:reach, self.columns(head)] = gq_t.T.astype(BF16)
            for (lo, hi), a, b in zip(pieces, first, second):
                gk = dot_nn(a, self.qh_ref[head, 0, off:reach]) + dot_nn(
                    b, self.qh_ref[head, 1, off:reach]
                )
                if lo == off:
                    self.gk_acc[lo:hi, :] = gk
                else:
                    self.gk_acc[lo:hi, :] += gk
        self.gk_ref[:, self.columns(head)] = self.gk_acc[...].astype(BF16)
        self.gl_ref[head] = jnp.broadcast_to(
            jnp.sum(lambda_total, axis=1, keepdims=True), self.gl_ref.shape[1:]
        )


def whole_kernel(
    n, m,
    lam_in, tok_ref, cot_ref, w_ref, q_ref, k_ref,
    gq_ref, gk_ref, gt_ref, gw_ref, glo_ref,
    lam_ref, qf, kf,
    vt_ref, gt_f, wct, tokens, tok_t, wc, coth, vloc, v_ref, p_ref, a_ref, qh_ref, kt_ref, go_ref, sum_acc,
    gvb, dv, part, ry, sz, rz, rzd, tokx, acc, sb, rc, sc, rd, gl_ref, lbuf,
    local_sem, send_sem, wa_r, wx_r, wd_r, tz_r, ty_r,
    c_r, v_r, dv_r, y_r, z_r, zd_r, tx_r, gx_r, gd_r, e_r,
    d_r, l_r,
):
    me = lax.axis_index("sp")
    dp = lax.axis_index("dp")
    place = n // 2
    levels = place // 2
    spans = m // 2
    half, pos = me // place, me % place
    level, y = pos // 2, pos % 2
    x, core = dp // 2, dp % 2
    rows, depth = tok_ref.shape
    length, heads, width = q_ref.shape
    feats = heads * width
    part_rows = rows // CHUNKS
    partner = (1 - half) * place + pos
    beside = me + 1 - 2 * y
    other = dp + 1 - 2 * core

    def at_pos(p):
        return half * place + p

    ups = [(level + k) % levels for k in range(1, levels)]
    xs = [(x + k) % spans for k in range(1, spans)]
    in_half = [(pos + k) % place for k in range(1, place)]
    sp_peers = [(me + k) % n for k in range(1, n)]
    dp_peers = [(dp + k) % m for k in range(1, m)]
    sent = []
    unit = p_ref.shape[3] * 4
    limit = p_ref.shape[2] * unit

    def size_of(ref):
        return math.prod(ref.shape) * jnp.dtype(ref.dtype).itemsize

    def wait_bytes(sem, size):
        if size <= limit:
            ref = p_ref.at[0, 0, pl.ds(0, size // unit)]
        else:
            ref = p_ref.at[0, :, pl.ds(0, size // unit // 2)]
        pltpu.make_async_copy(ref, ref, sem).wait()

    def send(src, dst, recv, sp, dp):
        size = size_of(src)
        if not sent or sent[-1] + size > limit:
            sent.append(0)
        sent[-1] += size
        return remote(src, dst, send_sem.at[len(sent) - 1], recv, sp, dp)

    def lane(start, size):
        return pl.ds(pl.multiple_of(start, size), size)

    locals_ = [
        pltpu.make_async_copy(tok_ref, tokens.at[pos], local_sem.at[0]),
        pltpu.make_async_copy(cot_ref.at[:, lane(me * feats, feats)], coth.at[me], local_sem.at[1]),
    ] + [
        pltpu.make_async_copy(
            w_ref.at[:, lane((j * place + pos) * feats, feats)],
            wc.at[me, dp, :, pl.ds(j * feats, feats)],
            local_sem.at[2 + j],
        )
        for j in range(2)
    ] + [
        pltpu.make_async_copy(q_ref, gq_ref, local_sem.at[4]),
        pltpu.make_async_copy(k_ref, gk_ref, local_sem.at[5]),
        pltpu.make_async_copy(lam_in, lam_ref, local_sem.at[6]),
    ]
    greet([(s, dp) for s in sp_peers] + [(me, d) for d in dp_peers], locals_)

    def begin(copy):
        copy.start()
        return copy

    def weight_out(k, s, j):
        start = (j * place + s % place) * feats
        return begin(
            send(
                w_ref.at[:, lane(start, feats)],
                wc.at[me, dp, :, pl.ds(j * feats, feats)],
                wa_r.at[min(k, place)],
                s,
                dp,
            )
        )

    def chunk(c):
        return pl.ds(c * part_rows, part_rows)

    def tok_up(k, c):
        return begin(
            send(
                tok_ref.at[chunk(c)],
                tokens.at[pos, chunk(c)],
                tz_r.at[k, c],
                at_pos(ups[k] * 2 + y),
                dp,
            )
        )

    def tok_side(slot, origin, c):
        src = tok_ref.at[chunk(c)] if slot == 0 else tokens.at[origin, chunk(c)]
        return begin(
            send(
                src,
                tokens.at[origin, chunk(c)],
                ty_r.at[slot],
                beside,
                dp,
            )
        )

    def cot_out(k, s):
        return send(
            cot_ref.at[:, lane(s * feats, feats)], coth.at[me], c_r.at[0], s, dp
        )

    far = [(1 - half) * place + (pos + k) % place for k in range(place)]
    near = [at_pos(p) for p in in_half]
    wa = [weight_out(place + k, s, j) for k, s in enumerate(near) for j in range(2)]
    wb = [[weight_out(k, s, j) for j in range(2)] for k, s in enumerate(far)]
    up, side = {}, {}
    for c in range(CHUNKS):
        for k in range(levels - 1):
            up[k, c] = tok_up(k, c)
    own = [tok_side(0, pos, c) for c in range(CHUNKS)]
    far_cots = [
        cot_out(
            2 * j + i,
            (1 - half) * place
            + (j + half * (levels - 1 - 2 * j)) * 2
            + (y if i == 0 else 1 - y),
        )
        for j in range(levels)
        for i in range(2)
    ]
    near_cots = [cot_out(place + k, s) for k, s in enumerate(near)]
    for copy in far_cots:
        copy.start()
    att = Attention(
        lam_ref, qf, kf, v_ref, coth,
        (p_ref, a_ref, qh_ref, kt_ref, go_ref, sum_acc, sum_acc, vt_ref, gt_f),
        (qf, kf, gl_ref), width,
    )
    for copy in locals_[4:]:
        copy.wait()
    qf[...] = gq_ref[...].reshape(length, feats)
    kf[...] = gk_ref[...].reshape(length, feats)
    pieces = [(h, i) for h in range(heads) for i in range(att.count)]
    for h in range(heads):
        att.prepare(h)
    first = len(pieces) // 2
    for h, i in pieces[:first]:
        att.softmaxes(h, i)

    def wc_block(h, p, d):
        return wc.at[h * place + p, d]

    for copy in locals_[2:4]:
        copy.wait()
    piece = size_of(w_ref) // n
    wait_bytes(wa_r.at[place], piece * len(wa))
    wx, wd = {}, []

    def core_out(slot, p, block):
        wd.append(
            begin(send(block, block, wd_r.at[0], me, other))
        )

    def x_out(j, p, block):
        for k, xk in enumerate(xs):
            wx[j, k, p] = begin(
                send(
                    block, block, wx_r.at[j, k, p], me, xk * 2 + core
                )
            )

    for p in range(place):
        block = wc_block(half, p, dp)
        x_out(0, p, block)
        core_out(0, p, block)
    for h, i in pieces[first:]:
        att.softmaxes(h, i)
    downs = [(level + levels - k - 1) % levels for k in range(levels - 1)]
    x_downs = [(x + spans - k - 1) % spans for k in range(spans - 1)]

    def side_on(c):
        for k in range(levels - 1):
            up[k, c].wait_recv()
            side[k, c] = tok_side(k + 1, downs[k] * 2 + y, c)

    count = w_ref.shape[0]
    txs = {}

    def turn(slot, b):
        turned = tokens[b].astype(F32).T.astype(BF16).reshape(2, place, m, count, rows)
        for h in range(2):
            for p in range(place):
                tok_t[b, p, h] = turned[h, p]
        stretch = lane((dp * place + b) * rows, rows)
        for k, d in enumerate(dp_peers):
            txs[k, slot] = begin(
                send(
                    tok_t.at[b, :, :, d],
                    tokx.at[:, :, :, stretch],
                    tx_r.at[0],
                    me,
                    d,
                )
            )
        tokx[:, :, :, stretch] = tok_t[b, :, :, dp]

    def x_on(j, p):
        for k, origin in enumerate(x_downs):
            wx[j, k, p].wait_recv()
            slot = (1 + k) if j == 0 else (spans + 1 + k)
            h, q = (half, p) if j == 0 else (1 - half, (pos + place - p) % place)
            core_out(slot, p, wc_block(h, q, origin * 2 + core))

    for k in range(place):
        wait_bytes(wa_r.at[k], piece * len(wb[k]))
        block = wc_block(1 - half, (pos + place - k) % place, dp)
        x_out(1, k, block)
        core_out(spans, k, block)
    for p in range(place):
        x_on(0, p)
    locals_[0].wait()
    for c in range(CHUNKS):
        side_on(c)
        if c == 0:
            turn(0, pos)
        if c == CHUNKS // 2 - 1:
            for p in range(place):
                x_on(1, p)
    for copy in near_cots:
        copy.start()
    for k in range(levels - 1):
        turn(1 + k, downs[k] * 2 + y)
    wait_bytes(ty_r.at[0], size_of(tok_ref))
    turn(levels, level * 2 + 1 - y)
    wait_bytes(wd_r.at[0], 2 * piece * len(wd))

    def weight():
        return wc[...].reshape(depth, 2 * feats)

    def values_of(b, k):
        vloc[b] = dot_nn(tokens[b], weight()).astype(BF16)
        v_ref[half, b] = vloc[b, :, lane(half * feats, feats)]

    def values_out(blocks):
        for h in range(heads):
            for b, k in blocks:
                v_copies[h, k] = begin(
                    send(
                        vloc.at[b, :, lane((1 - half) * feats + h * width, width)],
                        v_ref.at[half, b, :, pl.ds(h * width, width)],
                        v_r.at[h],
                        partner,
                        dp,
                    )
                )

    v_copies = {}
    blocks = (
        [(pos, 0)]
        + [(downs[k] * 2 + y, 1 + k) for k in range(levels - 1)]
        + [(level * 2 + 1 - y, levels)]
    )
    for b, k in blocks:
        values_of(b, k)
    values_out(blocks)
    wct[...] = weight().astype(F32).T.astype(BF16)
    for k in range(levels - 1):
        wait_bytes(ty_r.at[1 + k], size_of(tok_ref))
        b = downs[k] * 2 + 1 - y
        values_of(b, levels + 1 + k)
        values_out([(b, levels + 1 + k)])

    for k in range(levels - 1):
        turn(levels + 1 + k, downs[k] * 2 + 1 - y)
    locals_[1].wait()
    wait_bytes(c_r.at[0], size_of(cot_ref) // n * (n - 1))
    for h in range(heads):
        att.turn_cotangent(h)
    for h in range(heads):
        att.turn_values(h, half)

    order = (
        [u * 2 + 1 - y for u in ups] + [level * 2 + 1 - y] + [u * 2 + y for u in ups] + [pos]
    )
    dv_copies = {}

    def dv_out(h, k):
        dv_copies[h, k] = begin(
            send(
                gvb.at[h, 1 - half, order[k]],
                dv.at[dp, order[k], :, lane(half * feats + h * width, width)],
                dv_r.at[k],
                partner,
                dp,
            )
        )

    for h in range(heads):
        wait_bytes(v_r.at[h], size_of(v_ref) // 2 // heads)
        att.turn_values(h, 1 - half)
        att.values_grad(h)
        gvb[h] = sum_acc[...].astype(BF16).reshape(2, place, rows, width)
        dv_out(h, 0)
    for h in range(heads):
        for b in range(place):
            dv[dp, b, :, lane(half * feats + h * width, width)] = gvb[h, half, b]

    gxs, gds = {}, {}

    def share(d, j):
        if j == 0:
            return dv.at[d, :, :, lane(half * feats, feats)]
        return dv.at[d, order[j - 1], :, lane((1 - half) * feats, feats)]

    def share_core(slot, j, d):
        gds[slot, j] = begin(
            send(share(d, j), share(d, j), gd_r.at[min(j, 1)], me, other)
        )

    def share_out(j):
        for k, xk in enumerate(xs):
            gxs[k, j] = begin(
                send(
                    share(dp, j),
                    share(dp, j),
                    gx_r.at[k, j],
                    me,
                    xk * 2 + core,
                )
            )
        share_core(0, j, dp)

    def share_on(j):
        for k, origin in enumerate(x_downs):
            gxs[k, j].wait_recv()
            share_core(1 + k, j, origin * 2 + core)

    share_out(0)
    split = (heads + 1) // 2

    def dv_more():
        for h in range(heads):
            for k in range(1, levels):
                dv_out(h, k)

    for h in range(split):
        att.scores_grad(h, dv_more if h == 0 else None)

    def dv_wait(k):
        wait_bytes(dv_r.at[k], rows * feats * 2)
        share_out(1 + k)

    def partial(k):
        part[order[k]] = dot_nn(dv[dp, order[k]], wct[...]).astype(BF16)

    ys, zs, zd = {}, {}, {}
    last = CHUNKS - 1

    def y_out(k, c):
        ys[k, c] = begin(
            send(
                part.at[order[k], chunk(c)],
                ry.at[k, chunk(c)],
                y_r.at[min(k * CHUNKS + c, (levels - 1) * CHUNKS)],
                beside,
                dp,
            )
        )

    for k in range(levels):
        dv_wait(k)
        if k == 0:
            for h in range(heads):
                for j in range(levels, 2 * levels):
                    dv_out(h, j)
        partial(k)
        for c in range(last):
            y_out(k, c)
        if k < levels - 1:
            zd[k] = begin(
                send(
                    part.at[order[k], chunk(last)],
                    rzd.at[k],
                    zd_r.at[k],
                    at_pos(ups[k] * 2 + y),
                    dp,
                )
            )
    for h in range(split, heads):
        att.scores_grad(h)
    ls = [
        begin(remote(gl_ref, lbuf.at[k], send_sem.at[7], l_r.at[0], me, d))
        for k, d in enumerate(dp_peers)
    ]
    def last_out():
        total = part[order[levels - 1], chunk(last)].astype(F32)
        for k in range(levels - 1):
            zd[k].wait_recv()
            total = total + rzd[k].astype(F32)
        part[order[levels - 1], chunk(last)] = total.astype(BF16)
        y_out(levels - 1, last)

    def rows_up(c):
        for k in range(levels - 1):
            total = part[ups[k] * 2 + y, chunk(c)].astype(F32)
            if c < last:
                ys[k, c].wait_recv()
                total = total + ry[k, chunk(c)].astype(F32)
            sz[k, chunk(c)] = total.astype(BF16)
            zs[k, c] = begin(
                send(
                    sz.at[k, chunk(c)],
                    rz.at[k, chunk(c)],
                    z_r.at[k],
                    at_pos(ups[k] * 2 + y),
                    dp,
                )
            )

    share_on(0)
    for k in range(levels, 2 * levels - 1):
        dv_wait(k)
        partial(k)
    rows_up(last)
    rows_up(0)
    last_out()
    dv_wait(2 * levels - 1)
    wait_bytes(tx_r.at[0], size_of(tokx) // m * (m - 1))
    wait_bytes(gd_r.at[0], size_of(dv) // 2 // m * spans)

    es, ds_ = {}, {}
    turns = in_half + [pos]

    def term(j, side_half):
        cols = lane(side_half * feats, feats)
        total = dot_nn(
            tokx[...].reshape(place * 2 * count, m * place * rows),
            dv[:, :, :, cols].reshape(m * place * rows, feats),
        )
        acc[:, :, :, cols] = total.reshape(place, 2, count, feats)
        for k, p in enumerate(turns):
            sb[p, :, cols] = acc[p, 1 - half, :, cols].astype(BF16)
            es[j, k] = begin(
                send(
                    sb.at[p, :, cols], rc.at[p, :, cols], e_r.at[k], partner, dp
                )
            )

    term(0, half)
    for j in range(1, place):
        share_on(j)
    for c in range(1, last - 1):
        rows_up(c)
    share_on(place)
    wait_bytes(gd_r.at[1], size_of(dv) // 2 // m * spans)
    term(1, 1 - half)
    rows_up(last - 1)
    partial(2 * levels - 1)

    def finish(k):
        p = turns[k]
        wait_bytes(e_r.at[k], size_of(rc) // place)
        total = (acc[p, half] + rc[p].astype(F32)).astype(BF16)
        if k < place - 1:
            sc[p] = total
            ds_[k] = begin(
                send(sc.at[p], rd.at[pos], d_r.at[0], at_pos(p), dp)
            )
        else:
            rd[pos] = total

    gq_ref[...] = qf[...].reshape(gq_ref.shape)
    gk_ref[...] = kf[...].reshape(gk_ref.shape)
    for k in range(place):
        finish(k)
    wait_bytes(y_r.at[(levels - 1) * CHUNKS], size_of(tok_ref))
    total = part[pos].astype(F32) + ry[levels - 1].astype(F32)
    for k in range(levels - 1):
        wait_bytes(z_r.at[k], size_of(tok_ref))
        total = total + rz[k].astype(F32)
    gt_ref[...] = total.astype(BF16)
    lam = gl_ref[...]
    pltpu.make_async_copy(lbuf, lbuf, l_r.at[0]).wait()
    for k in range(m - 1):
        lam = lam + lbuf[k]
    glo_ref[...] = lam
    wait_bytes(d_r.at[0], size_of(rd) // place * (place - 1))
    for p in range(place):
        for j in range(2):
            start = (j * place + p) * feats
            gw_ref[:, start : start + feats] = rd[p, :, j * feats : (j + 1) * feats].astype(F32)
    pltpu.make_async_copy(lbuf, lbuf, send_sem.at[7]).wait()
    for g, size in enumerate(sent):
        wait_bytes(send_sem.at[g], size)


def finish_kernel(gq_ref, gk_ref, gt_ref, gw_ref, gl_ref, *refs):
    outs, lam_out, sems = refs[:4], refs[4], refs[5]
    copies = [
        pltpu.make_async_copy(src, dst, sems.at[i])
        for i, (src, dst) in enumerate(zip((gq_ref, gk_ref, gt_ref, gw_ref), outs))
    ]
    for copy in copies:
        copy.start()
    for h in range(gl_ref.shape[0]):
        lam_out[h] = jnp.max(gl_ref[h])
    for copy in copies:
        copy.wait()


def finish(gq, gk, gt, gw, gl):
    vmem = pl.BlockSpec(memory_space=pltpu.VMEM)
    hbm = pl.BlockSpec(memory_space=pltpu.HBM)
    results = [gq, gk, gt, gw]
    return pl.pallas_call(
        finish_kernel,
        out_shape=[jax.ShapeDtypeStruct(a.shape, a.dtype) for a in results]
        + [jax.ShapeDtypeStruct(gl.shape[:1], F32)],
        in_specs=[vmem] * 5,
        out_specs=[hbm] * 4 + [pl.BlockSpec(memory_space=pltpu.SMEM)],
        scratch_shapes=[pltpu.SemaphoreType.DMA((4,))],
        compiler_params=pltpu.CompilerParams(vmem_limit_bytes=2 * 1024 * 1024),
        name="finish",
    )(*results, gl)


def run(lambdas, tokens, cotangent, weight, queries, keys, n, m):
    rows, depth = tokens.shape
    count, features = weight.shape
    length, heads, width = queries.shape
    feats = heads * width
    place, levels, spans = n // 2, n // 4, m // 2
    block = min(QBLOCK, length)
    blocks = length // block
    tri = block * (blocks * (blocks + 1) // 2)
    vmem = pl.BlockSpec(memory_space=pltpu.VMEM)
    hbm = pl.BlockSpec(memory_space=pltpu.HBM)
    pair = 2 * feats

    def b16(*shape):
        return pltpu.VMEM(shape, BF16)

    def f32(*shape):
        return pltpu.VMEM(shape, F32)

    def dma(*shape):
        return [pltpu.SemaphoreType.DMA(tuple(max(s, 1) for s in shape))]

    scratch = (
        [
            pltpu.SMEM((heads,), F32),
            b16(length, feats),
            b16(length, feats),
            b16(heads, width, length),
            f32(heads, width, length),
            b16(pair, depth),
            b16(place, rows, depth),
            b16(place, place, 2, m, count, rows),
            b16(n, m, count, pair),
            b16(n, rows, feats),
            b16(place, rows, pair),
            b16(2, place, rows, feats),
            f32(heads, 2, tri, block),
            b16(heads, tri, block),
            b16(heads, 2, length, width),
            b16(heads, 2, width, length),
            b16(heads, width, length),
            f32(length, width),
            b16(heads, 2, place, rows, width),
            b16(m, place, rows, pair),
            b16(place, rows, depth),
            b16(levels, rows, depth),
            b16(max(levels - 1, 1), rows, depth),
            b16(max(levels - 1, 1), rows, depth),
            b16(max(levels - 1, 1), rows // CHUNKS, depth),
            b16(place, 2, count, m * place * rows),
            f32(place, 2, count, pair),
            b16(place, count, pair),
            b16(place, count, pair),
            b16(place, count, pair),
            b16(place, count, pair),
            f32(heads, 8, 128),
            f32(m - 1, heads, 8, 128),
            pltpu.SemaphoreType.DMA((7,)),
        ]
        + dma(8)
        + dma(place + 1)
        + dma(2, spans - 1, place)
        + dma(1)
        + dma(levels - 1, CHUNKS)
        + dma(levels)
        + dma(1)
        + dma(heads)
        + dma(place)
        + dma((levels - 1) * CHUNKS + 1)
        + dma(levels - 1)
        + dma(levels - 1)
        + dma(1)
        + dma(spans - 1, place + 1)
        + dma(2)
        + dma(place)
        + dma(1)
        + dma(1)
    )
    held = sum(
        math.prod(ref.shape) * jnp.dtype(ref.dtype).itemsize
        for ref in scratch
        if ref.memory_space == pltpu.VMEM
    )
    return pl.pallas_call(
        functools.partial(whole_kernel, n, m),
        out_shape=[
            jax.ShapeDtypeStruct((length, heads, width), BF16),
            jax.ShapeDtypeStruct((length, heads, width), BF16),
            jax.ShapeDtypeStruct((rows, depth), BF16),
            jax.ShapeDtypeStruct((count, features), F32),
            jax.ShapeDtypeStruct((heads, 8, 128), F32),
        ],
        in_specs=[pl.BlockSpec(memory_space=pltpu.HBM if heads > 1 else pl.ANY), hbm, hbm, hbm, hbm, hbm],
        out_specs=[vmem] * 5,
        scratch_shapes=scratch,
        compiler_params=pltpu.CompilerParams(
            collective_id=0, has_side_effects=True, vmem_limit_bytes=held + 8 * 1024 * 1024
        ),
        name="whole",
    )(lambdas, tokens, cotangent, weight, queries, keys)


def body(n, m, tokens, cotangent, value_weight, query_heads, key_heads, lambdas):
    large = [tokens[0], cotangent[0], value_weight, query_heads[0], key_heads[0]]
    if lambdas.size > 1:
        large = [lambdas] + large
    large = [pltpu.with_memory_space_constraint(a, pltpu.HBM) for a in large]
    if lambdas.size == 1:
        large = [lambdas] + large
    results = run(*large, n, m)
    grad_query, grad_key, grad_tokens, grad_weight, grad_lambda = finish(*results)
    return grad_query[None], grad_key[None], grad_tokens[None], grad_weight, grad_lambda


def solution(mesh):
    placed = (
        P("dp", "sp", None),
        P("dp", "sp", None),
        P(("sp", "dp"), None),
        P("dp", None, "sp", None),
        P("dp", None, "sp", None),
        P("sp"),
    )
    return jax.shard_map(
        functools.partial(body, mesh.shape["sp"], mesh.shape["dp"]),
        mesh=mesh,
        in_specs=placed,
        out_specs=(
            P("dp", None, "sp", None),
            P("dp", None, "sp", None),
            P("dp", "sp", None),
            P(("sp", "dp"), None),
            P("sp"),
        ),
        check_vma=False,
    )
```

```python
import functools
import math

import jax
import jax.numpy as jnp
from jax import lax
from jax.experimental import pallas as pl
from jax.experimental.pallas import tpu as pltpu
from jax.sharding import PartitionSpec as P

QBLOCK = 256
EPS = 1e-06
NEGATIVE = -1e30
CHUNKS = 4
F32 = jnp.float32
BF16 = jnp.bfloat16


def dot_nn(a, b):
    return jnp.dot(a, b, preferred_element_type=F32)


def dot_nt(a, b):
    return lax.dot_general(a, b, (((1,), (1,)), ((), ())), preferred_element_type=F32)


def remote(src, dst, send, recv, sp, dp):
    return pltpu.make_async_remote_copy(
        src_ref=src,
        dst_ref=dst,
        send_sem=send,
        recv_sem=recv,
        device_id=(sp, dp),
        device_id_type=pl.DeviceIdType.MESH,
    )


def greet(peers, copies):
    barrier = pltpu.get_barrier_semaphore()
    for sp, dp in peers:
        pl.semaphore_signal(
            barrier, inc=1, device_id=(sp, dp), device_id_type=pl.DeviceIdType.MESH
        )
    for copy in copies:
        copy.start()
    pl.semaphore_wait(barrier, len(peers))


class Attention:
    def __init__(self, lam_ref, q_ref, k_ref, v_ref, g_ref, bufs, outs, width):
        self.lam_ref, self.q_ref, self.k_ref = lam_ref, q_ref, k_ref
        self.v_ref, self.g_ref, self.width = v_ref, g_ref, width
        self.p_ref, self.a_ref, self.qh_ref, self.kt_ref, self.go_ref = bufs[:5]
        self.gv_acc, self.gk_acc, self.vt_ref, self.gt_ref = bufs[5:]
        self.gq_ref, self.gk_ref, self.gl_ref = outs
        self.length = q_ref.shape[0]
        self.block = min(QBLOCK, self.length)
        self.count = self.length // self.block

    def span(self, index):
        off = index * self.block
        reach = off + self.block
        pieces = ([(0, off)] if off else []) + [(off, reach)]
        base = self.block * (index * (index + 1) // 2)
        return off, reach, pieces, base

    def columns(self, head):
        return slice(head * self.width, (head + 1) * self.width)

    def prepare(self, head):
        length, width = self.length, self.width
        half = width // 2
        scaling = half ** (-0.5)
        lanes = lax.broadcasted_iota(jnp.int32, (length, width), 1)
        first_half = lanes < half
        q_all = self.q_ref[:, self.columns(head)].astype(F32) * scaling
        k_all = self.k_ref[:, self.columns(head)].astype(F32) * scaling
        self.qh_ref[head, 0] = jnp.where(first_half, q_all, 0.0).astype(BF16)
        self.qh_ref[head, 1] = jnp.where(first_half, 0.0, q_all).astype(BF16)
        self.kt_ref[head, 0] = jnp.where(first_half, k_all, 0.0).T.astype(BF16)
        self.kt_ref[head, 1] = jnp.where(first_half, 0.0, k_all).T.astype(BF16)

    def softmaxes(self, head, index):
        block = self.block
        lam = self.lam_ref[head]
        keep = lax.broadcasted_iota(jnp.int32, (block, block), 0) <= lax.broadcasted_iota(
            jnp.int32, (block, block), 1
        )
        off, reach, pieces, base = self.span(index)
        probs = []
        for c in range(2):
            qc = self.qh_ref[head, c, off:reach]
            scores = [dot_nt(self.k_ref[lo:hi, self.columns(head)], qc) for lo, hi in pieces]
            scores[-1] = jnp.where(keep, scores[-1], NEGATIVE)
            top = functools.reduce(
                jnp.maximum, [jnp.max(s, axis=0, keepdims=True) for s in scores]
            )
            exps = [jnp.exp(s - top) for s in scores]
            total = sum(jnp.sum(e, axis=0, keepdims=True) for e in exps)
            inv = 1.0 / total
            probs.append([e * inv for e in exps])
            for (lo, hi), p in zip(pieces, probs[c]):
                self.p_ref[head, c, base + lo : base + hi] = p
        for (lo, hi), p1, p2 in zip(pieces, *probs):
            self.a_ref[head, base + lo : base + hi] = (p1 - lam * p2).astype(BF16)

    def turn_cotangent(self, head):
        wide = self.g_ref[:, :, self.columns(head)].reshape(self.length, self.width)
        self.gt_ref[head] = wide.astype(F32).T

    def turn_values(self, head, half):
        size = self.length // 2
        span = pl.ds(pl.multiple_of(half * size, size), size)
        values = self.v_ref[half, :, :, self.columns(head)].reshape(size, self.width)
        self.vt_ref[head, :, span] = values.astype(F32).T.astype(BF16)

    def values_grad(self, head):
        for index in range(self.count):
            off, reach, pieces, base = self.span(index)
            weights = self.a_ref[head, base : base + reach]
            out_t = dot_nn(self.vt_ref[head, :, :reach], weights)
            cot = self.gt_ref[head, :, off:reach]
            inverse = lax.rsqrt(jnp.mean(out_t * out_t, axis=0, keepdims=True) + EPS)
            normed = out_t * inverse
            grad_out = (
                inverse * (cot - normed * jnp.mean(cot * normed, axis=0, keepdims=True))
            ).astype(BF16)
            self.go_ref[head, :, off:reach] = grad_out
            gv = dot_nt(weights, grad_out)
            if off:
                self.gv_acc[0:off] += gv[0:off]
            self.gv_acc[off:reach] = gv[off:reach]

    def scores_grad(self, head, midway=None):
        block, width = self.block, self.width
        lam = self.lam_ref[head]
        v_all = self.v_ref[:, :, :, self.columns(head)].reshape(self.length, width)
        lambda_total = jnp.zeros((1, block), F32)
        for index in range(self.count):
            if midway and index == self.count - 1:
                midway()
            off, reach, pieces, base = self.span(index)
            grad_out = self.go_ref[head, :, off:reach]
            probs = [
                [self.p_ref[head, c, base + lo : base + hi] for lo, hi in pieces]
                for c in range(2)
            ]
            grad_w = [dot_nn(v_all[lo:hi], grad_out) for lo, hi in pieces]
            sums = [
                sum(jnp.sum(d * p, axis=0, keepdims=True) for d, p in zip(grad_w, probs[c]))
                for c in range(2)
            ]
            lambda_total = lambda_total - sums[1]
            first = [(p * (d - sums[0])).astype(BF16) for d, p in zip(grad_w, probs[0])]
            second = [(-lam * p * (d - sums[1])).astype(BF16) for d, p in zip(grad_w, probs[1])]
            gq_t = sum(
                dot_nn(self.kt_ref[head, 0, :, lo:hi], a)
                + dot_nn(self.kt_ref[head, 1, :, lo:hi], b)
                for (lo, hi), a, b in zip(pieces, first, second)
            )
            self.gq_ref[off:reach, self.columns(head)] = gq_t.T.astype(BF16)
            for (lo, hi), a, b in zip(pieces, first, second):
                gk = dot_nn(a, self.qh_ref[head, 0, off:reach]) + dot_nn(
                    b, self.qh_ref[head, 1, off:reach]
                )
                if lo == off:
                    self.gk_acc[lo:hi, :] = gk
                else:
                    self.gk_acc[lo:hi, :] += gk
        self.gk_ref[:, self.columns(head)] = self.gk_acc[...].astype(BF16)
        self.gl_ref[head] = jnp.broadcast_to(
            jnp.sum(lambda_total, axis=1, keepdims=True), self.gl_ref.shape[1:]
        )


def whole_kernel(
    n, m,
    lam_in, tok_ref, cot_ref, w_ref, q_ref, k_ref,
    gq_ref, gk_ref, gt_ref, gw_ref, glo_ref,
    lam_ref, qf, kf,
    vt_ref, gt_f, wct, tokens, tok_t, wc, coth, vloc, v_ref, p_ref, a_ref, qh_ref, kt_ref, go_ref, sum_acc,
    gvb, dv, part, ry, sz, rz, tokx, acc, sb, rc, sc, rd, gl_ref, lbuf,
    local_sem, send_sem, wa_r, wx_r, wd_r, tz_r, ty_r,
    c_r, v_r, dv_r, y_r, z_r, tx_r, gx_r, gd_r, e_r,
    d_r, l_r,
):
    me = lax.axis_index("sp")
    dp = lax.axis_index("dp")
    place = n // 2
    levels = place // 2
    spans = m // 2
    half, pos = me // place, me % place
    level, y = pos // 2, pos % 2
    x, core = dp // 2, dp % 2
    rows, depth = tok_ref.shape
    length, heads, width = q_ref.shape
    feats = heads * width
    part_rows = rows // CHUNKS
    partner = (1 - half) * place + pos
    beside = me + 1 - 2 * y
    other = dp + 1 - 2 * core

    def at_pos(p):
        return half * place + p

    ups = [(level + k) % levels for k in range(1, levels)]
    xs = [(x + k) % spans for k in range(1, spans)]
    in_half = [(pos + k) % place for k in range(1, place)]
    sp_peers = [(me + k) % n for k in range(1, n)]
    dp_peers = [(dp + k) % m for k in range(1, m)]
    sent = []
    unit = p_ref.shape[3] * 4
    limit = p_ref.shape[2] * unit

    def size_of(ref):
        return math.prod(ref.shape) * jnp.dtype(ref.dtype).itemsize

    def wait_bytes(sem, size):
        if size <= limit:
            ref = p_ref.at[0, 0, pl.ds(0, size // unit)]
        else:
            ref = p_ref.at[0, :, pl.ds(0, size // unit // 2)]
        pltpu.make_async_copy(ref, ref, sem).wait()

    def send(src, dst, recv, sp, dp):
        size = size_of(src)
        if not sent or sent[-1] + size > limit:
            sent.append(0)
        sent[-1] += size
        return remote(src, dst, send_sem.at[len(sent) - 1], recv, sp, dp)

    def lane(start, size):
        return pl.ds(pl.multiple_of(start, size), size)

    locals_ = [
        pltpu.make_async_copy(tok_ref, tokens.at[pos], local_sem.at[0]),
        pltpu.make_async_copy(cot_ref.at[:, lane(me * feats, feats)], coth.at[me], local_sem.at[1]),
    ] + [
        pltpu.make_async_copy(
            w_ref.at[:, lane((j * place + pos) * feats, feats)],
            wc.at[me, dp, :, pl.ds(j * feats, feats)],
            local_sem.at[2 + j],
        )
        for j in range(2)
    ] + [
        pltpu.make_async_copy(q_ref, gq_ref, local_sem.at[4]),
        pltpu.make_async_copy(k_ref, gk_ref, local_sem.at[5]),
        pltpu.make_async_copy(lam_in, lam_ref, local_sem.at[6]),
    ]
    greet([(s, dp) for s in sp_peers] + [(me, d) for d in dp_peers], locals_)

    def begin(copy):
        copy.start()
        return copy

    def weight_out(k, s, j):
        start = (j * place + s % place) * feats
        return begin(
            send(
                w_ref.at[:, lane(start, feats)],
                wc.at[me, dp, :, pl.ds(j * feats, feats)],
                wa_r.at[min(k, place)],
                s,
                dp,
            )
        )

    def chunk(c):
        return pl.ds(c * part_rows, part_rows)

    def tok_up(k, c):
        return begin(
            send(
                tok_ref.at[chunk(c)],
                tokens.at[pos, chunk(c)],
                tz_r.at[k, c],
                at_pos(ups[k] * 2 + y),
                dp,
            )
        )

    def tok_side(slot, origin, c):
        src = tok_ref.at[chunk(c)] if slot == 0 else tokens.at[origin, chunk(c)]
        return begin(
            send(
                src,
                tokens.at[origin, chunk(c)],
                ty_r.at[slot],
                beside,
                dp,
            )
        )

    def cot_out(k, s):
        return send(
            cot_ref.at[:, lane(s * feats, feats)], coth.at[me], c_r.at[0], s, dp
        )

    far = [(1 - half) * place + (pos + k) % place for k in range(place)]
    near = [at_pos(p) for p in in_half]
    wa = [weight_out(place + k, s, j) for k, s in enumerate(near) for j in range(2)]
    wb = [[weight_out(k, s, j) for j in range(2)] for k, s in enumerate(far)]
    up, side = {}, {}
    for c in range(CHUNKS):
        for k in range(levels - 1):
            up[k, c] = tok_up(k, c)
    own = [tok_side(0, pos, c) for c in range(CHUNKS)]
    far_cots = [
        cot_out(
            2 * j + i,
            (1 - half) * place
            + (j + half * (levels - 1 - 2 * j)) * 2
            + (y if i == 0 else 1 - y),
        )
        for j in range(levels)
        for i in range(2)
    ]
    near_cots = [cot_out(place + k, s) for k, s in enumerate(near)]
    for copy in far_cots:
        copy.start()
    att = Attention(
        lam_ref, qf, kf, v_ref, coth,
        (p_ref, a_ref, qh_ref, kt_ref, go_ref, sum_acc, sum_acc, vt_ref, gt_f),
        (qf, kf, gl_ref), width,
    )
    for copy in locals_[4:]:
        copy.wait()
    qf[...] = gq_ref[...].reshape(length, feats)
    kf[...] = gk_ref[...].reshape(length, feats)
    pieces = [(h, i) for h in range(heads) for i in range(att.count)]
    for h in range(heads):
        att.prepare(h)
    first = len(pieces) // 2
    for h, i in pieces[:first]:
        att.softmaxes(h, i)

    def wc_block(h, p, d):
        return wc.at[h * place + p, d]

    for copy in locals_[2:4]:
        copy.wait()
    piece = size_of(w_ref) // n
    wait_bytes(wa_r.at[place], piece * len(wa))
    wx, wd = {}, []

    def core_out(slot, p, block):
        wd.append(
            begin(send(block, block, wd_r.at[0], me, other))
        )

    def x_out(j, p, block):
        for k, xk in enumerate(xs):
            wx[j, k, p] = begin(
                send(
                    block, block, wx_r.at[j, k, p], me, xk * 2 + core
                )
            )

    for p in range(place):
        block = wc_block(half, p, dp)
        x_out(0, p, block)
        core_out(0, p, block)
    for h, i in pieces[first:]:
        att.softmaxes(h, i)
    downs = [(level + levels - k - 1) % levels for k in range(levels - 1)]
    x_downs = [(x + spans - k - 1) % spans for k in range(spans - 1)]

    def side_on(c):
        for k in range(levels - 1):
            up[k, c].wait_recv()
            side[k, c] = tok_side(k + 1, downs[k] * 2 + y, c)

    count = w_ref.shape[0]
    txs = {}

    def turn(slot, b):
        turned = tokens[b].astype(F32).T.astype(BF16).reshape(2, place, m, count, rows)
        for h in range(2):
            for p in range(place):
                tok_t[b, p, h] = turned[h, p]
        stretch = lane((dp * place + b) * rows, rows)
        for k, d in enumerate(dp_peers):
            txs[k, slot] = begin(
                send(
                    tok_t.at[b, :, :, d],
                    tokx.at[:, :, :, stretch],
                    tx_r.at[0],
                    me,
                    d,
                )
            )
        tokx[:, :, :, stretch] = tok_t[b, :, :, dp]

    def x_on(j, p):
        for k, origin in enumerate(x_downs):
            wx[j, k, p].wait_recv()
            slot = (1 + k) if j == 0 else (spans + 1 + k)
            h, q = (half, p) if j == 0 else (1 - half, (pos + place - p) % place)
            core_out(slot, p, wc_block(h, q, origin * 2 + core))

    for k in range(place):
        wait_bytes(wa_r.at[k], piece * len(wb[k]))
        block = wc_block(1 - half, (pos + place - k) % place, dp)
        x_out(1, k, block)
        core_out(spans, k, block)
    for p in range(place):
        x_on(0, p)
    locals_[0].wait()
    for c in range(CHUNKS):
        side_on(c)
        if c == 0:
            turn(0, pos)
        if c == CHUNKS // 2 - 1:
            for p in range(place):
                x_on(1, p)
    for copy in near_cots:
        copy.start()
    for k in range(levels - 1):
        turn(1 + k, downs[k] * 2 + y)
    wait_bytes(ty_r.at[0], size_of(tok_ref))
    turn(levels, level * 2 + 1 - y)
    wait_bytes(wd_r.at[0], 2 * piece * len(wd))

    def weight():
        return wc[...].reshape(depth, 2 * feats)

    def values_of(b, k):
        vloc[b] = dot_nn(tokens[b], weight()).astype(BF16)
        v_ref[half, b] = vloc[b, :, lane(half * feats, feats)]

    def values_out(blocks):
        for h in range(heads):
            for b, k in blocks:
                v_copies[h, k] = begin(
                    send(
                        vloc.at[b, :, lane((1 - half) * feats + h * width, width)],
                        v_ref.at[half, b, :, pl.ds(h * width, width)],
                        v_r.at[h],
                        partner,
                        dp,
                    )
                )

    v_copies = {}
    blocks = (
        [(pos, 0)]
        + [(downs[k] * 2 + y, 1 + k) for k in range(levels - 1)]
        + [(level * 2 + 1 - y, levels)]
    )
    for b, k in blocks:
        values_of(b, k)
    values_out(blocks)
    wct[...] = weight().astype(F32).T.astype(BF16)
    for k in range(levels - 1):
        wait_bytes(ty_r.at[1 + k], size_of(tok_ref))
        b = downs[k] * 2 + 1 - y
        values_of(b, levels + 1 + k)
        values_out([(b, levels + 1 + k)])

    for k in range(levels - 1):
        turn(levels + 1 + k, downs[k] * 2 + 1 - y)
    locals_[1].wait()
    wait_bytes(c_r.at[0], size_of(cot_ref) // n * (n - 1))
    for h in range(heads):
        att.turn_cotangent(h)
    for h in range(heads):
        att.turn_values(h, half)

    order = (
        [u * 2 + 1 - y for u in ups] + [level * 2 + 1 - y] + [u * 2 + y for u in ups] + [pos]
    )
    dv_copies = {}

    def dv_out(h, k):
        dv_copies[h, k] = begin(
            send(
                gvb.at[h, 1 - half, order[k]],
                dv.at[dp, order[k], :, lane(half * feats + h * width, width)],
                dv_r.at[k],
                partner,
                dp,
            )
        )

    for h in range(heads):
        wait_bytes(v_r.at[h], size_of(v_ref) // 2 // heads)
        att.turn_values(h, 1 - half)
        att.values_grad(h)
        gvb[h] = sum_acc[...].astype(BF16).reshape(2, place, rows, width)
        dv_out(h, 0)
    for h in range(heads):
        for b in range(place):
            dv[dp, b, :, lane(half * feats + h * width, width)] = gvb[h, half, b]

    gxs, gds = {}, {}

    def share(d, j):
        if j == 0:
            return dv.at[d, :, :, lane(half * feats, feats)]
        return dv.at[d, order[j - 1], :, lane((1 - half) * feats, feats)]

    def share_core(slot, j, d):
        gds[slot, j] = begin(
            send(share(d, j), share(d, j), gd_r.at[min(j, 1)], me, other)
        )

    def share_out(j):
        for k, xk in enumerate(xs):
            gxs[k, j] = begin(
                send(
                    share(dp, j),
                    share(dp, j),
                    gx_r.at[k, j],
                    me,
                    xk * 2 + core,
                )
            )
        share_core(0, j, dp)

    def share_on(j):
        for k, origin in enumerate(x_downs):
            gxs[k, j].wait_recv()
            share_core(1 + k, j, origin * 2 + core)

    share_out(0)
    split = (heads + 1) // 2

    def dv_more():
        for h in range(heads):
            for k in range(1, levels):
                dv_out(h, k)

    for h in range(split):
        att.scores_grad(h, dv_more if h == 0 else None)

    def dv_wait(k):
        wait_bytes(dv_r.at[k], rows * feats * 2)
        share_out(1 + k)

    def partial(k):
        part[order[k]] = dot_nn(dv[dp, order[k]], wct[...]).astype(BF16)

    ys, zs = {}, {}

    def y_out(k, c):
        ys[k, c] = begin(
            send(
                part.at[order[k], chunk(c)],
                ry.at[k, chunk(c)],
                y_r.at[min(k * CHUNKS + c, (levels - 1) * CHUNKS)],
                beside,
                dp,
            )
        )

    for k in range(levels):
        dv_wait(k)
        if k == 0:
            for h in range(heads):
                for j in range(levels, 2 * levels):
                    dv_out(h, j)
        partial(k)
        for c in range(CHUNKS):
            y_out(k, c)
    for h in range(split, heads):
        att.scores_grad(h)
    ls = [
        begin(remote(gl_ref, lbuf.at[k], send_sem.at[7], l_r.at[0], me, d))
        for k, d in enumerate(dp_peers)
    ]
    def rows_up(c):
        for k in range(levels - 1):
            total = part[ups[k] * 2 + y, chunk(c)].astype(F32)
            ys[k, c].wait_recv()
            total = total + ry[k, chunk(c)].astype(F32)
            sz[k, chunk(c)] = total.astype(BF16)
            zs[k, c] = begin(
                send(
                    sz.at[k, chunk(c)],
                    rz.at[k, chunk(c)],
                    z_r.at[k],
                    at_pos(ups[k] * 2 + y),
                    dp,
                )
            )

    share_on(0)
    for k in range(levels, 2 * levels - 1):
        dv_wait(k)
        partial(k)
    rows_up(0)
    dv_wait(2 * levels - 1)
    wait_bytes(tx_r.at[0], size_of(tokx) // m * (m - 1))
    wait_bytes(gd_r.at[0], size_of(dv) // 2 // m * spans)

    es, ds_ = {}, {}
    turns = in_half + [pos]

    def term(j, side_half):
        cols = lane(side_half * feats, feats)
        total = dot_nn(
            tokx[...].reshape(place * 2 * count, m * place * rows),
            dv[:, :, :, cols].reshape(m * place * rows, feats),
        )
        acc[:, :, :, cols] = total.reshape(place, 2, count, feats)
        for k, p in enumerate(turns):
            sb[p, :, cols] = acc[p, 1 - half, :, cols].astype(BF16)
            es[j, k] = begin(
                send(
                    sb.at[p, :, cols], rc.at[p, :, cols], e_r.at[k], partner, dp
                )
            )

    term(0, half)
    for j in range(1, place):
        share_on(j)
    for c in range(1, CHUNKS - 1):
        rows_up(c)
    share_on(place)
    wait_bytes(gd_r.at[1], size_of(dv) // 2 // m * spans)
    term(1, 1 - half)
    rows_up(CHUNKS - 1)
    partial(2 * levels - 1)

    def finish(k):
        p = turns[k]
        wait_bytes(e_r.at[k], size_of(rc) // place)
        total = (acc[p, half] + rc[p].astype(F32)).astype(BF16)
        if k < place - 1:
            sc[p] = total
            ds_[k] = begin(
                send(sc.at[p], rd.at[pos], d_r.at[0], at_pos(p), dp)
            )
        else:
            rd[pos] = total

    gq_ref[...] = qf[...].reshape(gq_ref.shape)
    gk_ref[...] = kf[...].reshape(gk_ref.shape)
    for k in range(place):
        finish(k)
    wait_bytes(y_r.at[(levels - 1) * CHUNKS], size_of(tok_ref))
    total = part[pos].astype(F32) + ry[levels - 1].astype(F32)
    for k in range(levels - 1):
        wait_bytes(z_r.at[k], size_of(tok_ref))
        total = total + rz[k].astype(F32)
    gt_ref[...] = total.astype(BF16)
    lam = gl_ref[...]
    pltpu.make_async_copy(lbuf, lbuf, l_r.at[0]).wait()
    for k in range(m - 1):
        lam = lam + lbuf[k]
    glo_ref[...] = lam
    wait_bytes(d_r.at[0], size_of(rd) // place * (place - 1))
    for p in range(place):
        for j in range(2):
            start = (j * place + p) * feats
            gw_ref[:, start : start + feats] = rd[p, :, j * feats : (j + 1) * feats].astype(F32)
    pltpu.make_async_copy(lbuf, lbuf, send_sem.at[7]).wait()
    for g, size in enumerate(sent):
        wait_bytes(send_sem.at[g], size)


def finish_kernel(gq_ref, gk_ref, gt_ref, gw_ref, gl_ref, *refs):
    outs, lam_out, sems = refs[:4], refs[4], refs[5]
    copies = [
        pltpu.make_async_copy(src.at[part], dst.at[part], sems.at[2 * i + j])
        for i, (src, dst) in enumerate(zip((gq_ref, gk_ref, gt_ref, gw_ref), outs))
        for j in range(2)
        for part in [pl.ds(j * (src.shape[0] // 2), src.shape[0] // 2)]
    ]
    for copy in copies:
        copy.start()
    for h in range(gl_ref.shape[0]):
        lam_out[h] = jnp.max(gl_ref[h])
    for copy in copies:
        copy.wait()


def finish(gq, gk, gt, gw, gl):
    vmem = pl.BlockSpec(memory_space=pltpu.VMEM)
    hbm = pl.BlockSpec(memory_space=pltpu.HBM)
    results = [gq, gk, gt, gw]
    return pl.pallas_call(
        finish_kernel,
        out_shape=[jax.ShapeDtypeStruct(a.shape, a.dtype) for a in results]
        + [jax.ShapeDtypeStruct(gl.shape[:1], F32)],
        in_specs=[vmem] * 5,
        out_specs=[hbm] * 4 + [pl.BlockSpec(memory_space=pltpu.SMEM)],
        scratch_shapes=[pltpu.SemaphoreType.DMA((8,))],
        compiler_params=pltpu.CompilerParams(vmem_limit_bytes=2 * 1024 * 1024),
        name="finish",
    )(*results, gl)


def run(lambdas, tokens, cotangent, weight, queries, keys, n, m):
    rows, depth = tokens.shape
    count, features = weight.shape
    length, heads, width = queries.shape
    feats = heads * width
    place, levels, spans = n // 2, n // 4, m // 2
    block = min(QBLOCK, length)
    blocks = length // block
    tri = block * (blocks * (blocks + 1) // 2)
    vmem = pl.BlockSpec(memory_space=pltpu.VMEM)
    hbm = pl.BlockSpec(memory_space=pltpu.HBM)
    pair = 2 * feats

    def b16(*shape):
        return pltpu.VMEM(shape, BF16)

    def f32(*shape):
        return pltpu.VMEM(shape, F32)

    def dma(*shape):
        return [pltpu.SemaphoreType.DMA(tuple(max(s, 1) for s in shape))]

    scratch = (
        [
            pltpu.SMEM((heads,), F32),
            b16(length, feats),
            b16(length, feats),
            b16(heads, width, length),
            f32(heads, width, length),
            b16(pair, depth),
            b16(place, rows, depth),
            b16(place, place, 2, m, count, rows),
            b16(n, m, count, pair),
            b16(n, rows, feats),
            b16(place, rows, pair),
            b16(2, place, rows, feats),
            f32(heads, 2, tri, block),
            b16(heads, tri, block),
            b16(heads, 2, length, width),
            b16(heads, 2, width, length),
            b16(heads, width, length),
            f32(length, width),
            b16(heads, 2, place, rows, width),
            b16(m, place, rows, pair),
            b16(place, rows, depth),
            b16(levels, rows, depth),
            b16(max(levels - 1, 1), rows, depth),
            b16(max(levels - 1, 1), rows, depth),
            b16(place, 2, count, m * place * rows),
            f32(place, 2, count, pair),
            b16(place, count, pair),
            b16(place, count, pair),
            b16(place, count, pair),
            b16(place, count, pair),
            f32(heads, 8, 128),
            f32(m - 1, heads, 8, 128),
            pltpu.SemaphoreType.DMA((7,)),
        ]
        + dma(8)
        + dma(place + 1)
        + dma(2, spans - 1, place)
        + dma(1)
        + dma(levels - 1, CHUNKS)
        + dma(levels)
        + dma(1)
        + dma(heads)
        + dma(place)
        + dma((levels - 1) * CHUNKS + 1)
        + dma(levels - 1)
        + dma(1)
        + dma(spans - 1, place + 1)
        + dma(2)
        + dma(place)
        + dma(1)
        + dma(1)
    )
    held = sum(
        math.prod(ref.shape) * jnp.dtype(ref.dtype).itemsize
        for ref in scratch
        if ref.memory_space == pltpu.VMEM
    )
    return pl.pallas_call(
        functools.partial(whole_kernel, n, m),
        out_shape=[
            jax.ShapeDtypeStruct((length, heads, width), BF16),
            jax.ShapeDtypeStruct((length, heads, width), BF16),
            jax.ShapeDtypeStruct((rows, depth), BF16),
            jax.ShapeDtypeStruct((count, features), F32),
            jax.ShapeDtypeStruct((heads, 8, 128), F32),
        ],
        in_specs=[pl.BlockSpec(memory_space=pltpu.HBM if heads > 1 else pl.ANY), hbm, hbm, hbm, hbm, hbm],
        out_specs=[vmem] * 5,
        scratch_shapes=scratch,
        compiler_params=pltpu.CompilerParams(
            collective_id=0, has_side_effects=True, vmem_limit_bytes=held + 8 * 1024 * 1024
        ),
        name="whole",
    )(lambdas, tokens, cotangent, weight, queries, keys)


def body(n, m, tokens, cotangent, value_weight, query_heads, key_heads, lambdas):
    large = [tokens[0], cotangent[0], value_weight, query_heads[0], key_heads[0]]
    if lambdas.size > 1:
        large = [lambdas] + large
    large = [pltpu.with_memory_space_constraint(a, pltpu.HBM) for a in large]
    if lambdas.size == 1:
        large = [lambdas] + large
    results = run(*large, n, m)
    grad_query, grad_key, grad_tokens, grad_weight, grad_lambda = finish(*results)
    return grad_query[None], grad_key[None], grad_tokens[None], grad_weight, grad_lambda


def solution(mesh):
    placed = (
        P("dp", "sp", None),
        P("dp", "sp", None),
        P(("sp", "dp"), None),
        P("dp", None, "sp", None),
        P("dp", None, "sp", None),
        P("sp"),
    )
    return jax.shard_map(
        functools.partial(body, mesh.shape["sp"], mesh.shape["dp"]),
        mesh=mesh,
        in_specs=placed,
        out_specs=(
            P("dp", None, "sp", None),
            P("dp", None, "sp", None),
            P("dp", "sp", None),
            P(("sp", "dp"), None),
            P("sp"),
        ),
        check_vma=False,
    )
```
